32 devices in a mesh: ep: 8 (over z, core), tp: 4 (over y, x).
Axes of the slice: x: 2, y: 2, z: 4, core: 2. Of those that a mesh axis runs over, the one named last changes fastest.
Arguments:
- mixer_input: bfloat16 [1024, 2048], P('ep'), may hold values from -6 to 6
- mixer_gain: float32 [2048], replicated, may hold values from 0.1 to 1.9
- glu_value_weight: bfloat16 [512, 2048], P('tp'), may hold values from -0.125 to 0.125
- glu_gate_weight: bfloat16 [512, 2048], P('tp'), may hold values from -0.125 to 0.125
- conv_taps: float32 [512, 31], P('tp'), may hold values from -1 to 1
- conv_bias: float32 [512], P('tp'), may hold values from -3 to 3
- channel_gain: float32 [512], replicated, may hold values from 0.1 to 1.9
- channel_shift: float32 [512], replicated, may hold values from -3 to 3
- mixer_out_weight: bfloat16 [512, 2048], P(None, 'tp'), may hold values from -0.25 to 0.25
- expert_input: bfloat16 [2048, 2048], P('ep'), may hold values from -6 to 6
- expert_gain: float32 [2048], replicated, may hold values from 0.1 to 1.9
- routes: int32 [2048, 2], P('ep'), may hold values from 0 to 7, all different within a row; in each aligned block of 256 rows (0 to 255, 256 to 511, ...) at most 96 rows name the same one
- route_logits: float32 [2048, 2], P('ep'), may hold values from -8 to 8
- gate_weight: bfloat16 [8, 2048, 4096], P('ep', None, 'tp'), may hold values from -0.125 to 0.125
- up_weight: bfloat16 [8, 2048, 4096], P('ep', None, 'tp'), may hold values from -0.125 to 0.125
- down_weight: bfloat16 [8, 4096, 2048], P('ep', 'tp'), may hold values from -0.09375 to 0.09375
Outputs:
- mixer_output: bfloat16 [1024, 2048], P('ep', 'tp')
- expert_output: bfloat16 [2048, 2048], P('ep', 'tp')
The draws below stay inside these ranges and needn't reach their ends.
Inputs may be any that keep to these rules, and one draw needn't show every extreme that they name: `routes`: the 2 entries of a row differ. Among the rows of one index of ep, no expert is named by more than 96 rows, a bound that some block reaches.
All inputs are finite; a program needn't handle non-finite values.
Results may differ from the reference program's by a relative error of at most 0.015.
Values may be sent and summed in bfloat16 or wider, within the bound.
A program may use at most 64 MiB of HBM per device.

```python
import math
import jax
import jax.numpy as jnp
import numpy as np
from jax import lax

D = 2048
CH = 512
FF = 4096
KERNEL = 31
TOP = 2
ROWS_B = 256
EXPERTS = 8
CAP = 96
TOKENS_A = 1024
TOKENS_B = 2048
N_EP = 8
N_TP = 4


def shard_levels(own_key, extent, pieces, least, high):
    def one(axis_at, blocks):
        steps = jax.random.uniform(jax.random.fold_in(jax.random.fold_in(own_key, 6), axis_at), (blocks,), jnp.float32, least / len(pieces), high / len(pieces))
        return jnp.repeat(jnp.exp(steps), extent[axis_at] // blocks).reshape((-1,) + (1,) * (len(extent) - axis_at - 1))

    factor_of = one(*pieces[0])
    for cut in pieces[1:]:
        factor_of = factor_of * one(*cut)
    return factor_of


def assign_block(rng, own, number, rows, count, top, limit, skew):
    order = jax.random.permutation(rng, count)
    crowded, usual = portions_of(count, rows * top, limit, skew, True), portions_of(count, rows * top, limit, skew, False)
    places = jnp.arange(count)

    def named(sizes, rotation):
        used = int((sizes > 0).sum())
        fixed = max(1, used // 4)
        moved = fixed + (places - fixed + rotation * (used - fixed)) % max(1, count - fixed)
        return jnp.zeros((count,), jnp.int32).at[order[jnp.where(places < fixed, places, moved)]].set(jnp.asarray(sizes, jnp.int32))

    sizes = jnp.where(number % 4 == 0, named(crowded, number // 4), named(usual, number - number // 4 - 1))
    mixed = jax.random.permutation(jax.random.fold_in(own, 3), count)
    giver, sink = mixed[0:count // 2 * 2:2], mixed[1:count // 2 * 2:2]
    room = jnp.minimum(sizes[giver] - 1, limit - sizes[sink]) // 2
    room = jnp.where((giver == order[0]) | (sink == order[0]) | (sizes[sink] == 0), 0, jnp.maximum(room, 0))
    moved = jax.random.randint(jax.random.fold_in(own, 4), (count // 2,), 0, 1 << 20) % (room + 1)
    sizes = sizes.at[giver].add(-moved).at[sink].add(moved)
    labels = jnp.searchsorted(jnp.cumsum(sizes), jnp.arange(rows * top), side="right").astype(jnp.int32)
    listing = labels.reshape(top, rows).T
    listing = listing[jax.random.permutation(jax.random.fold_in(own, 1), rows)]
    rotation = jax.random.randint(jax.random.fold_in(own, 2), (rows, 1), 0, top)
    return jnp.take_along_axis(listing, (jnp.arange(top)[None, :] + rotation) % top, axis=1)


def portions_of(number_of, total, most, lean, full):
    portions = [(1 << 20) // math.isqrt(grade ** lean) + 1 for grade in range(1, number_of + 1)]
    largest = most if full else min(most, max(-(-total // number_of), total * portions[0] // sum(portions)))
    least = 1 if total - largest >= number_of - 1 else 0
    counts, surplus = [largest] + [least] * (number_of - 1), total - largest - least * (number_of - 1)
    while surplus > 0:
        free = [i for i in range(1, number_of) if counts[i] < largest] or [i for i in range(1, number_of) if counts[i] < most]
        pool, budget = sum([portions[i] for i in free]), surplus
        for i in free:
            extra = min(most - counts[i], max(1, budget * portions[i] // pool), surplus)
            counts[i] = counts[i] + extra
            surplus = surplus - extra
    return np.array(counts)


def noise(rng, dims, width, reach, split=(), kind=jnp.bfloat16):
    array = jax.random.normal(rng, dims, jnp.float32) * width
    if len(split) > 0:
        array = shard_levels(rng, dims, split, -0.22, 0.18) * array
    return jnp.clip(array, min=-reach, max=reach).astype(kind)


def setup_inputs(seed: int = 0) -> dict:
    key_list = jax.random.split(jax.random.key(seed), 17)
    mixer_input = noise(key_list[0], (TOKENS_A, D), 1.0, 6.0, ((0, 8),))
    mixer_gain = jnp.clip(1.0 + 0.18 * jax.random.normal(key_list[1], (D,), jnp.float32), 0.1, 1.9)
    glu_value_weight = noise(key_list[2], (CH, D), D ** -0.5, 0.125, ((0, 4),))
    glu_gate_weight = noise(key_list[3], (CH, D), D ** -0.5, 0.125, ((0, 4),))
    conv_taps = noise(key_list[4], (CH, KERNEL), KERNEL ** -0.5, 1.0, ((0, 4),), jnp.float32)
    conv_bias = noise(key_list[5], (CH,), 0.5, 3.0, ((0, 4),), jnp.float32)
    channel_gain = jnp.clip(1.0 + 0.18 * jax.random.normal(key_list[6], (CH,), jnp.float32), 0.1, 1.9)
    channel_shift = noise(key_list[7], (CH,), 0.5, 3.0, (), jnp.float32)
    mixer_out_weight = noise(key_list[8], (CH, D), CH ** -0.5, 0.25, ((1, 4),))
    expert_input = noise(key_list[9], (TOKENS_B, D), 1.0, 6.0, ((0, 8),))
    expert_gain = jnp.clip(1.0 + 0.18 * jax.random.normal(key_list[10], (D,), jnp.float32), 0.1, 1.9)
    routes_keys = jax.random.split(jax.random.fold_in(key_list[11], 1), TOKENS_B // ROWS_B)
    routes_turns = jax.random.permutation(jax.random.fold_in(key_list[11], 3), TOKENS_B // ROWS_B)
    routes = jax.vmap(lambda own, number: assign_block(jax.random.fold_in(key_list[11], 2), own, number, ROWS_B, EXPERTS, TOP, CAP, 1))(routes_keys, routes_turns).reshape((TOKENS_B, TOP))
    route_logits = noise(key_list[12], (TOKENS_B, TOP), 1.5, 8.0, ((0, 8),), jnp.float32)
    gate_weight = noise(key_list[13], (EXPERTS, D, FF), D ** -0.5, 0.125, ((0, 8), (2, 4)))
    up_weight = noise(key_list[14], (EXPERTS, D, FF), D ** -0.5, 0.125, ((0, 8), (2, 4)))
    down_weight = noise(key_list[15], (EXPERTS, FF, D), FF ** -0.5, 0.09375, ((0, 8), (1, 4)))
    return {"mixer_input": mixer_input, "mixer_gain": mixer_gain, "glu_value_weight": glu_value_weight, "glu_gate_weight": glu_gate_weight, "conv_taps": conv_taps, "conv_bias": conv_bias, "channel_gain": channel_gain, "channel_shift": channel_shift, "mixer_out_weight": mixer_out_weight, "expert_input": expert_input, "expert_gain": expert_gain, "routes": routes, "route_logits": route_logits, "gate_weight": gate_weight, "up_weight": up_weight, "down_weight": down_weight}


norm_eps = 1e-06

def rms_rows(row_block, gain_vec):
    row_values = row_block.astype(jnp.float32)
    inv_scale = lax.rsqrt(lax.optimization_barrier(jnp.mean(row_values * row_values, axis=-1, keepdims=True)) + norm_eps)
    return (row_values * inv_scale * gain_vec[None, :]).astype(jnp.bfloat16)

def mixer_half(mixer_input, mixer_gain, glu_value_weight, glu_gate_weight, conv_taps, conv_bias, channel_gain, channel_shift, mixer_out_weight):
    normed = rms_rows(mixer_input, mixer_gain)
    contract = (((1,), (1,)), ((), ()))
    glu_value = lax.dot_general(normed, glu_value_weight, contract, preferred_element_type=jnp.float32)
    glu_gate = lax.dot_general(normed, glu_gate_weight, contract, preferred_element_type=jnp.float32)
    gated_rows = (glu_value * jax.nn.sigmoid(glu_gate)).astype(jnp.bfloat16)
    padded = jnp.pad(gated_rows.astype(jnp.float32), ((KERNEL - 1, 0), (0, 0)))
    conv_sum = jnp.zeros((TOKENS_A, CH), jnp.float32)
    for offset in range(KERNEL):
        conv_sum = conv_sum + padded[offset:offset + TOKENS_A] * conv_taps[:, offset][None, :]
    conv_out = (conv_sum + conv_bias[None, :]).astype(jnp.bfloat16)
    chan_values = conv_out.astype(jnp.float32)
    chan_mean = lax.optimization_barrier(jnp.mean(chan_values, axis=1, keepdims=True))
    centered = chan_values - chan_mean
    variance = lax.optimization_barrier(jnp.mean(centered * centered, axis=1, keepdims=True))
    shaped = centered * lax.rsqrt(variance + norm_eps) * channel_gain[None, :] + channel_shift[None, :]
    activated = jax.nn.silu(shaped).astype(jnp.bfloat16)
    return jnp.dot(activated, mixer_out_weight, preferred_element_type=jnp.float32).astype(jnp.bfloat16)

def expert_half(expert_input, expert_gain, routes, route_logits, gate_weight, up_weight, down_weight):
    normed = rms_rows(expert_input, expert_gain)
    assigned = routes.reshape(N_EP, ROWS_B * TOP)
    matches = (assigned[:, :, None] == jnp.arange(EXPERTS, dtype=jnp.int32)[None, None, :]).astype(jnp.int32)
    earlier = jnp.cumsum(matches, axis=1) - matches
    slot_index = lax.optimization_barrier(jnp.sum(earlier * matches, axis=2))
    source_dev = jnp.arange(N_EP, dtype=jnp.int32)[:, None]
    slot_place = (source_dev * CAP + slot_index).reshape(-1).astype(jnp.int32)
    owner_row = (source_dev * ROWS_B + jnp.arange(ROWS_B * TOP, dtype=jnp.int32)[None, :] // TOP).reshape(-1).astype(jnp.int32)
    expert_ids = assigned.reshape(-1)
    slot_owner = jnp.full((EXPERTS, N_EP * CAP), TOKENS_B, jnp.int32).at[expert_ids, slot_place].set(owner_row)

    def one_expert(packed):
        slot_rows, gate_mat, up_mat, down_mat = packed
        rows_in = jnp.take(normed, slot_rows, axis=0, mode='fill', fill_value=0)
        gate_acts = jnp.dot(rows_in, gate_mat, preferred_element_type=jnp.float32)
        up_acts = jnp.dot(rows_in, up_mat, preferred_element_type=jnp.float32)
        hidden = (jax.nn.silu(gate_acts) * up_acts).astype(jnp.bfloat16)
        hid_groups = hidden.reshape(N_EP * CAP, N_TP, FF // N_TP).astype(jnp.float32)
        down_groups = down_mat.reshape(N_TP, FF // N_TP, D).astype(jnp.float32)
        partial_value = jnp.einsum('sgf,gfd->gsd', hid_groups, down_groups).astype(jnp.bfloat16)
        return lax.optimization_barrier(jnp.sum(partial_value.astype(jnp.float32), axis=0)).astype(jnp.bfloat16)
    results = lax.map(one_expert, (slot_owner, gate_weight, up_weight, down_weight))
    picked = results[expert_ids, slot_place].astype(jnp.float32).reshape(TOKENS_B, TOP, D)
    first_weight = jax.nn.sigmoid(route_logits[:, 0] - route_logits[:, 1])
    second_weight = jax.nn.sigmoid(route_logits[:, 1] - route_logits[:, 0])
    combined = picked[:, 0] * first_weight[:, None] + picked[:, 1] * second_weight[:, None]
    return combined.astype(jnp.bfloat16)

def reference(mixer_input, mixer_gain, glu_value_weight, glu_gate_weight, conv_taps, conv_bias, channel_gain, channel_shift, mixer_out_weight, expert_input, expert_gain, routes, route_logits, gate_weight, up_weight, down_weight):
    mixer_output = mixer_half(mixer_input, mixer_gain, glu_value_weight, glu_gate_weight, conv_taps, conv_bias, channel_gain, channel_shift, mixer_out_weight)
    expert_output = expert_half(expert_input, expert_gain, routes, route_logits, gate_weight, up_weight, down_weight)
    return (mixer_output, expert_output)
```

```python
import functools

import jax
import jax.numpy as jnp
from jax import lax
from jax.experimental import pallas as pl
from jax.experimental.pallas import tpu as pltpu
from jax.sharding import PartitionSpec as P

norm_eps = 1e-06
MESH = pl.DeviceIdType.MESH
f32 = jnp.float32
bf16 = jnp.bfloat16


def step_kernel(
    n_ep, n_tp, cap,
    x_ref, gain_ref, routes_ref, routes_t_ref, logits_ref, gate_hbm, up_hbm, down_hbm,
    mix_gain_ref, taps_ref, bias_ref, chan_gain_ref, chan_shift_ref,
    mix_hbm, value_hbm, glu_gate_hbm, mix_out_hbm,
    out_ref, mix_out_ref,
    gate_w, up_w, down_w, normed, out_part, out_pair, xin, hidden, part, own_part, got, summed, ret,
    w_sem, z_send, z_recv, ag_send, ag_recv, rs_send, rs_recv, y_send, y_recv,
    mix_in, value_w, glu_gate_w, mix_out_w, gated, tail, padded, conv_own, channels,
    tail_sem, c_send, c_recv,
):
    e = lax.axis_index("ep")
    t = lax.axis_index("tp")
    n_z = n_ep // 2
    z = e // 2
    c = e % 2
    mate = e + 1 - 2 * c
    width = out_part.shape[1]
    rows, feat = x_ref.shape
    pair = 2 * cap
    slots = n_ep * cap
    peers = n_tp - 1

    weight_copies = [
        pltpu.make_async_copy(gate_hbm.at[0], gate_w, w_sem.at[0]),
        pltpu.make_async_copy(up_hbm.at[0], up_w, w_sem.at[1]),
        pltpu.make_async_copy(down_hbm.at[0], down_w, w_sem.at[2]),
    ]
    mix_copies = [
        pltpu.make_async_copy(mix_hbm, mix_in, w_sem.at[3]),
        pltpu.make_async_copy(value_hbm, value_w, w_sem.at[4]),
        pltpu.make_async_copy(glu_gate_hbm, glu_gate_w, w_sem.at[5]),
        pltpu.make_async_copy(mix_out_hbm, mix_out_w, w_sem.at[6]),
    ]
    for copy in mix_copies[:3] + weight_copies + mix_copies[3:]:
        copy.start()

    barrier = pltpu.get_barrier_semaphore()
    for o in range(1, n_ep):
        pl.semaphore_signal(barrier, inc=1, device_id=((e + o) % n_ep, t), device_id_type=MESH)
    for o in range(1, n_tp):
        pl.semaphore_signal(barrier, inc=1, device_id=(e, (t + o) % n_tp), device_id_type=MESH)

    def rows_of(index, count):
        return pl.ds(pl.multiple_of(index * count, count), count)

    def cols_of(index, count):
        return pl.ds(pl.multiple_of(index * count, count), count)

    values = x_ref[...].astype(f32)
    scale = lax.rsqrt(jnp.mean(values * values, axis=-1, keepdims=True) + norm_eps)
    normed[...] = (values * scale * gain_ref[...]).astype(bf16)

    lanes = lax.broadcasted_iota(jnp.int32, (rows, 128), 1)
    m0 = (lanes == routes_ref[:, 0:1]).astype(f32)
    m1 = (lanes == routes_ref[:, 1:2]).astype(f32)
    ri = lax.broadcasted_iota(jnp.int32, (rows, rows), 0)
    ci = lax.broadcasted_iota(jnp.int32, (rows, rows), 1)
    lower = (ci < ri).astype(f32).astype(bf16)
    upper = (ri < ci).astype(f32).astype(bf16)
    count = jnp.dot(lower, (m0 + m1).astype(bf16), preferred_element_type=f32)
    base = count + (lanes * cap).astype(f32)
    place0 = jnp.sum(base * m0, axis=1, keepdims=True).astype(jnp.int32)
    place1 = jnp.sum(base * m1, axis=1, keepdims=True).astype(jnp.int32)
    subs = lax.broadcasted_iota(jnp.int32, (128, rows), 0)
    t0 = (subs == routes_t_ref[0:1, :]).astype(f32)
    t1 = (subs == routes_t_ref[1:2, :]).astype(f32)
    count_t = jnp.dot((t0 + t1).astype(bf16), upper, preferred_element_type=f32)
    base_t = count_t + (subs * cap).astype(f32)
    row0 = jnp.sum(base_t * t0, axis=0, keepdims=True).astype(jnp.int32)
    row1 = jnp.sum(base_t * t1, axis=0, keepdims=True).astype(jnp.int32)

    def pick(first, size):
        at = lax.broadcasted_iota(jnp.int32, (size, rows), 0) + first
        return ((at == row0) | (at == row1)).astype(f32).astype(bf16)

    out_part[...] = jnp.dot(
        pick(0, slots), normed[:, cols_of(t, width)], preferred_element_type=f32
    ).astype(bf16)

    pl.semaphore_wait(barrier, n_ep - 1 + peers)

    z_copies = []
    for k in range(1, n_z):
        for cc in range(2):
            dest = ((z + k) % n_z) * 2 + cc
            copy = pltpu.make_async_remote_copy(
                src_ref=out_part.at[rows_of(dest, cap), :],
                dst_ref=xin.at[rows_of(e, cap), cols_of(t, width)],
                send_sem=z_send.at[2 * k + cc],
                recv_sem=z_recv.at[2 * k + c],
                device_id=(dest, t),
                device_id_type=MESH,
            )
            copy.start()
            z_copies.append(copy)

    out_pair[...] = jnp.dot(
        pick(mate * cap, cap), normed[...], preferred_element_type=f32
    ).astype(bf16)
    mate_copy = pltpu.make_async_remote_copy(
        src_ref=out_pair,
        dst_ref=xin.at[rows_of(e, cap), :],
        send_sem=z_send.at[0],
        recv_sem=z_recv.at[0],
        device_id=(mate, t),
        device_id_type=MESH,
    )
    mate_copy.start()
    xin[rows_of(e, cap), :] = jnp.dot(
        pick(e * cap, cap), normed[...], preferred_element_type=f32
    ).astype(bf16)

    def source_chip(k):
        return (z + n_z - k) % n_z

    ag_copies = []

    def gather(k):
        chip = source_chip(k)
        for cc in range(2):
            block = xin.at[rows_of(chip * 2 + cc, cap), cols_of(t, width)]
            pltpu.make_async_remote_copy(
                src_ref=block, dst_ref=block, send_sem=z_send.at[2 * k + cc],
                recv_sem=z_recv.at[2 * k + cc], device_id=(mate, t), device_id_type=MESH,
            ).wait_recv()
        block = xin.at[rows_of(chip, pair), cols_of(t, width)]
        for o in range(1, n_tp):
            copy = pltpu.make_async_remote_copy(
                src_ref=block, dst_ref=block, send_sem=ag_send.at[k * peers + o - 1],
                recv_sem=ag_recv.at[k * peers + o - 1],
                device_id=(e, (t + o) % n_tp), device_id_type=MESH,
            )
            copy.start()
            ag_copies.append(copy)

    def gathered(k):
        chip = source_chip(k)
        for o in range(1, n_tp):
            block = xin.at[rows_of(chip, pair), cols_of((t + n_tp - o) % n_tp, width)]
            pltpu.make_async_remote_copy(
                src_ref=block, dst_ref=block, send_sem=ag_send.at[k * peers + o - 1],
                recv_sem=ag_recv.at[k * peers + o - 1],
                device_id=(mate, t), device_id_type=MESH,
            ).wait_recv()

    units = gate_w.shape[1]
    tile = min(units, 256)
    rs_copies = []
    y_copies = []

    def up_half(k):
        here = rows_of(source_chip(k), pair)

        def one(j, carry):
            cols = cols_of(j, tile)
            rows_in = xin[here, :]
            g = jnp.dot(rows_in, gate_w[:, cols], preferred_element_type=f32)
            u = jnp.dot(rows_in, up_w[:, cols], preferred_element_type=f32)
            hidden[:, cols] = (g * jax.nn.sigmoid(g) * u).astype(bf16)
            return carry

        lax.fori_loop(0, units // tile, one, 0)

    def down_half(k):
        for o in range(1, n_tp):
            peer = (t + o) % n_tp
            at = k * peers + o - 1
            part[at] = jnp.dot(
                hidden[...], down_w[:, cols_of(peer, width)], preferred_element_type=f32
            ).astype(bf16)
            copy = pltpu.make_async_remote_copy(
                src_ref=part.at[at], dst_ref=got.at[at], send_sem=rs_send.at[at],
                recv_sem=rs_recv.at[at], device_id=(e, peer), device_id_type=MESH,
            )
            copy.start()
            rs_copies.append(copy)
        own_part[k] = jnp.dot(
            hidden[...], down_w[:, cols_of(t, width)], preferred_element_type=f32
        ).astype(bf16)

    def finish(k):
        chip = source_chip(k)
        total = own_part[k].astype(f32)
        for o in range(1, n_tp):
            at = k * peers + o - 1
            pltpu.make_async_remote_copy(
                src_ref=part.at[at], dst_ref=got.at[at], send_sem=rs_send.at[at],
                recv_sem=rs_recv.at[at], device_id=(mate, t), device_id_type=MESH,
            ).wait_recv()
            total = total + got[at].astype(f32)
        summed[k] = total.astype(bf16)
        if k == 0:
            copy = pltpu.make_async_remote_copy(
                src_ref=summed.at[0, rows_of(1 - c, cap), :], dst_ref=ret.at[rows_of(e, cap), :],
                send_sem=y_send.at[0], recv_sem=y_recv.at[0],
                device_id=(mate, t), device_id_type=MESH,
            )
            copy.start()
            y_copies.append(copy)
            ret[rows_of(e, cap), :] = summed[0, rows_of(c, cap), :]
            return
        for cc in range(2):
            copy = pltpu.make_async_remote_copy(
                src_ref=summed.at[k, pl.ds(cc * cap, cap), :], dst_ref=ret.at[rows_of(e, cap), :],
                send_sem=y_send.at[2 * k + cc], recv_sem=y_recv.at[2 * k + c],
                device_id=(chip * 2 + cc, t), device_id_type=MESH,
            )
            copy.start()
            y_copies.append(copy)

    taken, chans = gated.shape
    keep = tail.shape[0]
    reach = taps_ref.shape[0] - 1
    conv_copies = []

    def tail_copy():
        return pltpu.make_async_remote_copy(
            src_ref=gated.at[pl.ds(taken - keep, keep), :], dst_ref=tail,
            send_sem=tail_sem.at[0], recv_sem=tail_sem.at[1],
            device_id=((e + 1) % n_ep, t), device_id_type=MESH,
        )

    def glu():
        for copy in mix_copies[:3]:
            copy.wait()
        mixed = mix_in[...].astype(f32)
        inv = lax.rsqrt(jnp.mean(mixed * mixed, axis=-1, keepdims=True) + norm_eps)
        normed_a = (mixed * inv * mix_gain_ref[...]).astype(bf16)
        contract = (((1,), (1,)), ((), ()))
        value = lax.dot_general(normed_a, value_w[...], contract, preferred_element_type=f32)
        gate = lax.dot_general(normed_a, glu_gate_w[...], contract, preferred_element_type=f32)
        gated[...] = (value * jax.nn.sigmoid(gate)).astype(bf16)
        copy = tail_copy()
        copy.start()
        conv_copies.append(copy)

    def convolve():
        tail_copy().wait_recv()
        before = tail[...].astype(f32)
        padded[pl.ds(0, keep), :] = jnp.where(e > 0, before, jnp.zeros_like(before))
        padded[pl.ds(keep, taken), :] = gated[...].astype(f32)
        total = jnp.zeros((taken, chans), f32)
        for offset in range(reach + 1):
            shift = keep - reach + offset
            total = total + padded[pl.ds(shift, taken), :] * taps_ref[offset : offset + 1, :]
        done = (total + bias_ref[...]).astype(bf16)
        conv_own[...] = done
        channels[t] = done
        for o in range(1, n_tp):
            copy = pltpu.make_async_remote_copy(
                src_ref=conv_own, dst_ref=channels.at[t],
                send_sem=c_send.at[o - 1], recv_sem=c_recv.at[o - 1],
                device_id=(e, (t + o) % n_tp), device_id_type=MESH,
            )
            copy.start()
            conv_copies.append(copy)

    def mixer_end():
        for o in range(1, n_tp):
            pltpu.make_async_remote_copy(
                src_ref=conv_own, dst_ref=channels.at[(t + n_tp - o) % n_tp],
                send_sem=c_send.at[o - 1], recv_sem=c_recv.at[o - 1],
                device_id=(mate, t), device_id_type=MESH,
            ).wait_recv()
        mix_copies[3].wait()
        chan_values = jnp.concatenate([channels[i].astype(f32) for i in range(n_tp)], axis=1)
        centered = chan_values - jnp.mean(chan_values, axis=1, keepdims=True)
        variance = jnp.mean(centered * centered, axis=1, keepdims=True)
        shaped = (
            centered * lax.rsqrt(variance + norm_eps) * chan_gain_ref[...] + chan_shift_ref[...]
        )
        activated = (shaped * jax.nn.sigmoid(shaped)).astype(bf16)
        mix_out_ref[...] = jnp.dot(
            activated, mix_out_w[...], preferred_element_type=f32
        ).astype(bf16)

    glu()
    if n_z > 1:
        gather(1)
    mate_block = xin.at[rows_of(mate, cap), :]
    pltpu.make_async_remote_copy(
        src_ref=mate_block, dst_ref=mate_block, send_sem=z_send.at[0], recv_sem=z_recv.at[0],
        device_id=(mate, t), device_id_type=MESH,
    ).wait_recv()
    weight_copies[0].wait()
    weight_copies[1].wait()
    for k in range(n_z):
        if k > 0:
            gathered(k)
        up_half(k)
        if k == 0:
            weight_copies[2].wait()
        if k + 2 < n_z:
            gather(k + 2)
        down_half(k)
        if k == 0:
            convolve()
        if k > 0:
            finish(k - 1)
        if k == 1 or n_z == 1:
            mixer_end()
    finish(n_z - 1)

    block = ret.at[rows_of(mate, cap), :]
    pltpu.make_async_remote_copy(
        src_ref=block, dst_ref=block, send_sem=y_send.at[0], recv_sem=y_recv.at[0],
        device_id=(mate, t), device_id_type=MESH,
    ).wait_recv()
    for k in range(1, n_z):
        for cc in range(2):
            block = ret.at[rows_of(((z + k) % n_z) * 2 + cc, cap), :]
            pltpu.make_async_remote_copy(
                src_ref=block, dst_ref=block, send_sem=y_send.at[2 * k + cc],
                recv_sem=y_recv.at[2 * k + cc], device_id=(mate, t), device_id_type=MESH,
            ).wait_recv()
    at = lax.broadcasted_iota(jnp.int32, (rows, slots), 1)
    l0 = logits_ref[:, 0:1]
    l1 = logits_ref[:, 1:2]
    first = jnp.dot(
        (at == place0).astype(f32).astype(bf16), ret[...], preferred_element_type=f32
    )
    second = jnp.dot(
        (at == place1).astype(f32).astype(bf16), ret[...], preferred_element_type=f32
    )
    out_ref[...] = (
        first * jax.nn.sigmoid(l0 - l1) + second * jax.nn.sigmoid(l1 - l0)
    ).astype(bf16)
    for copy in [mate_copy] + z_copies + ag_copies + rs_copies + y_copies + conv_copies:
        copy.wait_send()


def paired_kernel(
    n_ep, n_tp, cap,
    x_hbm, gain_hbm, routes_hbm, logits_hbm, gate_hbm, up_hbm, down_hbm,
    mix_gain_hbm, taps_hbm, bias_hbm, chan_gain_hbm, chan_shift_hbm,
    mix_hbm, value_hbm, glu_gate_hbm, mix_out_hbm,
    out_ref, mix_out_ref,
    x_in, gain_in, routes_in, logits_in, gate_w, up_w, down_w,
    mix_gain_in, taps_in, bias_in, chan_gain_in, chan_shift_in,
    mix_in, value_w, glu_gate_w, mix_out_w,
    normed, columns, out_part, out_pair, xin, hidden,
    part_x, part_y, got_x, got_y, held_own, held_x, held_y, pass_x, pass_y, last_x, last_y,
    summed, ret, acc,
    load_sem, z_send, z_recv, ag_send, ag_recv, rs_send, rs_recv, y_send, y_recv,
    gated, tail, padded, conv_own, channels,
    tail_sem, c_send, c_recv,
):
    e = lax.axis_index("ep")
    t = lax.axis_index("tp")
    n_z = n_ep // 2
    z = e // 2
    c = e % 2
    mate = e + 1 - 2 * c
    rows, feat = x_in.shape
    width = out_part.shape[1]
    half = width // 2
    pair = 2 * cap
    slots = n_ep * cap
    units = gate_w.shape[1]
    tile = min(units, 256)
    tiles = units // tile
    t_x = t + 1 - 2 * (t % 2)
    t_y = (t + 2) % 4
    t_d = 3 - t

    def chip_of(k):
        return [z, z + 1 - 2 * (z % 2), (z + 2) % 4, 3 - z][k]

    def rows_of(index, count):
        return pl.ds(pl.multiple_of(index * count, count), count)

    def cols(quarter, first, count):
        return pl.ds(pl.multiple_of(quarter * width + first, 128), count)

    def load(src, dst, at):
        return pltpu.make_async_copy(src, dst, load_sem.at[at])

    def weight_tile(j):
        here = pl.ds(pl.multiple_of(j * tile, tile), tile)
        return (
            load(gate_hbm.at[0, :, here], gate_w.at[:, here], 16 + 2 * j),
            load(up_hbm.at[0, :, here], up_w.at[:, here], 17 + 2 * j),
        )

    load_routes = load(routes_hbm, routes_in, 0)
    load_logits = load(logits_hbm, logits_in, 1)
    load_gain = load(gain_hbm, gain_in, 2)
    load_x = load(x_hbm, x_in, 3)
    load_mix = [
        load(mix_hbm, mix_in, 4), load(mix_gain_hbm, mix_gain_in, 5),
        load(value_hbm, value_w, 6), load(glu_gate_hbm, glu_gate_w, 7),
    ]
    load_conv = [load(taps_hbm, taps_in, 8), load(bias_hbm, bias_in, 9)]
    load_end = [
        load(chan_gain_hbm, chan_gain_in, 10), load(chan_shift_hbm, chan_shift_in, 11),
        load(mix_out_hbm, mix_out_w, 12),
    ]
    load_down = load(down_hbm.at[0], down_w, 13)
    for copy in [load_x, load_gain, load_routes, load_logits] + load_mix + load_conv:
        copy.start()
    for j in range(tiles):
        for copy in weight_tile(j):
            copy.start()
    for copy in [load_down] + load_end:
        copy.start()

    barrier = pltpu.get_barrier_semaphore()
    for o in range(1, n_ep):
        pl.semaphore_signal(barrier, inc=1, device_id=((e + o) % n_ep, t), device_id_type=MESH)
    for o in range(1, n_tp):
        pl.semaphore_signal(barrier, inc=1, device_id=(e, (t + o) % n_tp), device_id_type=MESH)

    load_routes.wait()
    ri = lax.broadcasted_iota(jnp.int32, (rows, rows), 0)
    ci = lax.broadcasted_iota(jnp.int32, (rows, rows), 1)
    upper = (ri < ci).astype(f32).astype(bf16)
    subs = lax.broadcasted_iota(jnp.int32, (128, rows), 0)
    t0 = (subs == routes_in[0:1, :]).astype(f32)
    t1 = (subs == routes_in[1:2, :]).astype(f32)
    count_t = jnp.dot((t0 + t1).astype(bf16), upper, preferred_element_type=f32)
    base_t = count_t + (subs * cap).astype(f32)
    place0 = jnp.sum(base_t * t0, axis=0, keepdims=True)
    place1 = jnp.sum(base_t * t1, axis=0, keepdims=True)
    row0 = place0.astype(jnp.int32)
    row1 = place1.astype(jnp.int32)

    def pick(first, size):
        at = lax.broadcasted_iota(jnp.int32, (size, rows), 0) + first
        return ((at == row0) | (at == row1)).astype(f32).astype(bf16)

    load_x.wait()
    load_gain.wait()
    values = x_in[...].astype(f32)
    scale = lax.rsqrt(jnp.mean(values * values, axis=-1, keepdims=True) + norm_eps)
    normed[...] = (values * scale * gain_in[...]).astype(bf16)
    out_part[...] = jnp.dot(
        pick(0, slots), normed[:, cols(t, 0, width)], preferred_element_type=f32
    ).astype(bf16)

    pl.semaphore_wait(barrier, n_ep - 1 + n_tp - 1)

    sent = []

    def send(src, dst, send_sem, recv_sem, to):
        copy = pltpu.make_async_remote_copy(
            src_ref=src, dst_ref=dst, send_sem=send_sem, recv_sem=recv_sem,
            device_id=to, device_id_type=MESH,
        )
        copy.start()
        sent.append(copy)

    def arrive(dst, send_sem, recv_sem):
        pltpu.make_async_remote_copy(
            src_ref=dst, dst_ref=dst, send_sem=send_sem, recv_sem=recv_sem,
            device_id=(mate, t), device_id_type=MESH,
        ).wait_recv()

    for k in range(1, n_z):
        for cc in range(2):
            dest = chip_of(k) * 2 + cc
            send(
                out_part.at[rows_of(dest, cap), :], xin.at[rows_of(e, cap), cols(t, 0, width)],
                z_send.at[2 * k + cc], z_recv.at[2 * k + c], (dest, t),
            )

    out_pair[...] = jnp.dot(
        pick(mate * cap, cap), normed[...], preferred_element_type=f32
    ).astype(bf16)
    send(out_pair, xin.at[rows_of(e, cap), :], z_send.at[0], z_recv.at[0], (mate, t))
    xin[rows_of(e, cap), :] = jnp.dot(
        pick(e * cap, cap), normed[...], preferred_element_type=f32
    ).astype(bf16)

    def routed(k):
        for cc in range(2):
            arrive(
                xin.at[rows_of(chip_of(k) * 2 + cc, cap), cols(t, 0, width)],
                z_send.at[2 * k + cc], z_recv.at[2 * k + cc],
            )
        block = xin.at[rows_of(chip_of(k), pair), cols(t, 0, width)]
        send(block, block, ag_send.at[k - 1, 0], ag_recv.at[k - 1, 0], (e, t_x))
        send(block, block, ag_send.at[k - 1, 1], ag_recv.at[k - 1, 1], (e, t_y))

    def relay(k):
        here = rows_of(chip_of(k), pair)
        arrive(xin.at[here, cols(t_y, 0, width)], ag_send.at[k - 1, 1], ag_recv.at[k - 1, 1])
        block = xin.at[here, cols(t_y, 0, half)]
        send(block, block, ag_send.at[k - 1, 2], ag_recv.at[k - 1, 2], (e, t_x))
        arrive(xin.at[here, cols(t_x, 0, width)], ag_send.at[k - 1, 0], ag_recv.at[k - 1, 0])
        block = xin.at[here, cols(t_x, half, half)]
        send(block, block, ag_send.at[k - 1, 3], ag_recv.at[k - 1, 3], (e, t_y))

    def gathered(k):
        here = rows_of(chip_of(k), pair)
        arrive(xin.at[here, cols(t_d, 0, half)], ag_send.at[k - 1, 2], ag_recv.at[k - 1, 2])
        arrive(xin.at[here, cols(t_d, half, half)], ag_send.at[k - 1, 3], ag_recv.at[k - 1, 3])

    def up_half(k):
        here = rows_of(chip_of(k), pair)

        def one(j, carry):
            if k == 0:
                for copy in weight_tile(j):
                    copy.wait()
            at = pl.ds(pl.multiple_of(j * tile, tile), tile)
            rows_in = xin[here, :]
            g = jnp.dot(rows_in, gate_w[:, at], preferred_element_type=f32)
            u = jnp.dot(rows_in, up_w[:, at], preferred_element_type=f32)
            hidden[k, :, at] = (g * jax.nn.sigmoid(g) * u).astype(bf16)
            return carry

        lax.fori_loop(0, tiles, one, 0)

    def group(u):
        if u == 0:
            return 0, rows_of(1 - c, cap), pl.ds(0, cap)
        if u == n_z:
            return 0, rows_of(c, cap), pl.ds(cap, cap)
        return u, pl.ds(0, pair), pl.ds(0, pair)

    def down_half(u):
        k, here, at = group(u)

        def product(quarter):
            return jnp.dot(
                hidden[k, here, :], down_w[:, cols(quarter, 0, width)],
                preferred_element_type=f32,
            ).astype(bf16)

        def give(src, dst, way, to):
            send(src, dst, rs_send.at[u, way], rs_recv.at[u, way], (e, to))

        far = product(t_d)
        part_x[k, 1, at, :] = far[:, :half]
        part_y[k, 1, at, :] = far[:, half:]
        give(part_x.at[k, 1, at, :], got_x.at[k, 1, at, :], 0, t_x)
        give(part_y.at[k, 1, at, :], got_y.at[k, 1, at, :], 1, t_y)
        near = product(t_x)
        part_x[k, 0, at, :] = near[:, :half]
        held_x[k, at, :] = near[:, half:]
        give(part_x.at[k, 0, at, :], got_x.at[k, 0, at, :], 2, t_x)
        near = product(t_y)
        part_y[k, 0, at, :] = near[:, half:]
        held_y[k, at, :] = near[:, :half]
        give(part_y.at[k, 0, at, :], got_y.at[k, 0, at, :], 3, t_y)
        held_own[k, at, :] = product(t)

    def pass_on(u):
        k, here, at = group(u)
        arrive(got_x.at[k, 1, at, :], rs_send.at[u, 0], rs_recv.at[u, 0])
        pass_y[k, at, :] = (
            held_y[k, at, :].astype(f32) + got_x[k, 1, at, :].astype(f32)
        ).astype(bf16)
        send(
            pass_y.at[k, at, :], last_y.at[k, at, :], rs_send.at[u, 4], rs_recv.at[u, 4], (e, t_y)
        )
        arrive(got_y.at[k, 1, at, :], rs_send.at[u, 1], rs_recv.at[u, 1])
        pass_x[k, at, :] = (
            held_x[k, at, :].astype(f32) + got_y[k, 1, at, :].astype(f32)
        ).astype(bf16)
        send(
            pass_x.at[k, at, :], last_x.at[k, at, :], rs_send.at[u, 5], rs_recv.at[u, 5], (e, t_x)
        )

    def finish(u):
        k, here, at = group(u)
        arrive(got_x.at[k, 0, at, :], rs_send.at[u, 2], rs_recv.at[u, 2])
        arrive(got_y.at[k, 0, at, :], rs_send.at[u, 3], rs_recv.at[u, 3])
        arrive(last_y.at[k, at, :], rs_send.at[u, 4], rs_recv.at[u, 4])
        arrive(last_x.at[k, at, :], rs_send.at[u, 5], rs_recv.at[u, 5])
        low = (
            held_own[k, at, :half].astype(f32)
            + got_x[k, 0, at, :].astype(f32) + last_y[k, at, :].astype(f32)
        ).astype(bf16)
        high = (
            held_own[k, at, half:].astype(f32)
            + got_y[k, 0, at, :].astype(f32) + last_x[k, at, :].astype(f32)
        ).astype(bf16)
        if u == n_z:
            ret[rows_of(e, cap), :half] = low
            ret[rows_of(e, cap), half:] = high
            return
        summed[k, at, :half] = low
        summed[k, at, half:] = high
        if u == 0:
            send(
                summed.at[0, pl.ds(0, cap), :], ret.at[rows_of(e, cap), :],
                y_send.at[0], y_recv.at[0], (mate, t),
            )
            return
        for cc in range(2):
            send(
                summed.at[k, pl.ds(cc * cap, cap), :], ret.at[rows_of(e, cap), :],
                y_send.at[2 * k + cc], y_recv.at[2 * k + c], (chip_of(k) * 2 + cc, t),
            )

    def weighted(first, size):
        at = lax.broadcasted_iota(jnp.int32, (rows, size), 1) + first
        back = ret[rows_of(first // size, size), :]
        one = jnp.dot(
            (at == columns[0, :, 0:1].astype(jnp.int32)).astype(f32).astype(bf16), back,
            preferred_element_type=f32,
        )
        two = jnp.dot(
            (at == columns[1, :, 0:1].astype(jnp.int32)).astype(f32).astype(bf16), back,
            preferred_element_type=f32,
        )
        return one * columns[2, :, 0:1] + two * columns[3, :, 0:1]

    def returned(k):
        for cc in range(2):
            arrive(
                ret.at[rows_of(chip_of(k) * 2 + cc, cap), :],
                y_send.at[2 * k + cc], y_recv.at[2 * k + cc],
            )
        return weighted(chip_of(k) * pair, pair)

    taken, chans = gated.shape
    keep = tail.shape[0]
    reach = taps_in.shape[0] - 1

    def tail_refs():
        return gated.at[pl.ds(taken - keep, keep), :], tail, tail_sem.at[0], tail_sem.at[1]

    def glu():
        for copy in load_mix:
            copy.wait()
        mixed = mix_in[...].astype(f32)
        inv = lax.rsqrt(jnp.mean(mixed * mixed, axis=-1, keepdims=True) + norm_eps)
        normed_a = (mixed * inv * mix_gain_in[...]).astype(bf16)
        contract = (((1,), (1,)), ((), ()))
        value = lax.dot_general(normed_a, value_w[...], contract, preferred_element_type=f32)
        gate = lax.dot_general(normed_a, glu_gate_w[...], contract, preferred_element_type=f32)
        gated[...] = (value * jax.nn.sigmoid(gate)).astype(bf16)
        send(*tail_refs(), ((e + 1) % n_ep, t))

    def convolve():
        for copy in load_conv:
            copy.wait()
        arrive(tail, tail_sem.at[0], tail_sem.at[1])
        before = tail[...].astype(f32)
        padded[pl.ds(0, keep), :] = jnp.where(e > 0, before, jnp.zeros_like(before))
        padded[pl.ds(keep, taken), :] = gated[...].astype(f32)
        total = jnp.zeros((taken, chans), f32)
        for offset in range(reach + 1):
            shift = keep - reach + offset
            total = total + padded[pl.ds(shift, taken), :] * taps_in[offset : offset + 1, :]
        done = (total + bias_in[...]).astype(bf16)
        conv_own[...] = done
        channels[t] = done
        for o in range(1, n_tp):
            send(
                conv_own, channels.at[t], c_send.at[o - 1], c_recv.at[o - 1],
                (e, (t + o) % n_tp),
            )

    def mixer_end():
        for o in range(1, n_tp):
            arrive(channels.at[(t + n_tp - o) % n_tp], c_send.at[o - 1], c_recv.at[o - 1])
        for copy in load_end:
            copy.wait()
        chan_values = jnp.concatenate([channels[i].astype(f32) for i in range(n_tp)], axis=1)
        centered = chan_values - jnp.mean(chan_values, axis=1, keepdims=True)
        variance = jnp.mean(centered * centered, axis=1, keepdims=True)
        shaped = (
            centered * lax.rsqrt(variance + norm_eps) * chan_gain_in[...] + chan_shift_in[...]
        )
        activated = (shaped * jax.nn.sigmoid(shaped)).astype(bf16)
        mix_out_ref[...] = jnp.dot(
            activated, mix_out_w[...], preferred_element_type=f32
        ).astype(bf16)

    glu()
    arrive(xin.at[rows_of(mate, cap), :], z_send.at[0], z_recv.at[0])
    up_half(0)
    load_down.wait()
    down_half(0)
    routed(1)
    convolve()
    load_logits.wait()
    columns[0] = jnp.broadcast_to(place0, (128, rows)).T
    columns[1] = jnp.broadcast_to(place1, (128, rows)).T
    lead = logits_in[0:1, :] - logits_in[1:2, :]
    columns[2] = jnp.broadcast_to(jax.nn.sigmoid(lead), (128, rows)).T
    columns[3] = jnp.broadcast_to(jax.nn.sigmoid(-lead), (128, rows)).T
    pass_on(0)
    relay(1)
    finish(0)
    routed(2)
    gathered(1)
    up_half(1)
    relay(2)
    down_half(1)
    mixer_end()
    routed(3)
    pass_on(1)
    gathered(2)
    up_half(2)
    relay(3)
    down_half(2)
    finish(1)
    pass_on(2)
    gathered(3)
    up_half(3)
    down_half(3)
    finish(2)
    down_half(4)
    pass_on(3)
    acc[...] = returned(1)
    finish(3)
    pass_on(4)
    arrive(ret.at[rows_of(mate, cap), :], y_send.at[0], y_recv.at[0])
    acc[...] += returned(2) + weighted(mate * cap, cap)
    acc[...] += returned(3)
    finish(4)
    out_ref[...] = (acc[...] + weighted(e * cap, cap)).astype(bf16)
    for copy in sent:
        copy.wait_send()


def on_device(*args):
    n_ep, n_tp = lax.axis_size("ep"), lax.axis_size("tp")
    if n_tp == 4 and n_ep == 8:
        return paired_step(*args)
    return ring_step(*args)


def paired_step(
    mixer_input, mixer_gain, glu_value_weight, glu_gate_weight, conv_taps, conv_bias,
    channel_gain, channel_shift, mixer_out_weight, expert_input, expert_gain, routes,
    route_logits, gate_weight, up_weight, down_weight,
):
    n_ep, n_tp = lax.axis_size("ep"), lax.axis_size("tp")
    rows, feat = expert_input.shape
    cap = 3 * rows // n_ep
    cap = -(-cap // 16) * 16
    units = gate_weight.shape[2]
    width = feat // n_tp
    half = width // 2
    n_z, pair, slots = n_ep // 2, 2 * cap, n_ep * cap
    taken, chans, taps = mixer_input.shape[0], conv_taps.shape[0], conv_taps.shape[1]
    keep = -(-(taps - 1) // 16) * 16
    dma = pltpu.SemaphoreType.DMA
    operands = (
        expert_input, expert_gain[None, :], routes.T, route_logits.T,
        gate_weight, up_weight, down_weight,
        mixer_gain[None, :], conv_taps.T, conv_bias[None, :], channel_gain[None, :],
        channel_shift[None, :], mixer_input, glu_value_weight, glu_gate_weight, mixer_out_weight,
    )

    def held(array):
        shape = array.shape[1:] if array.ndim == 3 else array.shape
        return pltpu.VMEM(shape, array.dtype)

    block = pltpu.VMEM((n_z, pair, half), bf16)
    blocks = pltpu.VMEM((n_z, 2, pair, half), bf16)
    wide = pltpu.VMEM((n_z, pair, width), bf16)
    vmem = pl.BlockSpec(memory_space=pltpu.VMEM)
    expert_output, mixer_output = pl.pallas_call(
        functools.partial(paired_kernel, n_ep, n_tp, cap),
        out_shape=(
            jax.ShapeDtypeStruct((rows, width), bf16),
            jax.ShapeDtypeStruct((taken, mixer_out_weight.shape[1]), bf16),
        ),
        in_specs=[pl.BlockSpec(memory_space=pltpu.HBM)] * len(operands),
        out_specs=(vmem, vmem),
        scratch_shapes=[held(array) for array in operands] + [
            pltpu.VMEM((rows, feat), bf16),
            pltpu.VMEM((4, rows, 128), f32),
            pltpu.VMEM((slots, width), bf16),
            pltpu.VMEM((cap, feat), bf16),
            pltpu.VMEM((slots, feat), bf16),
            pltpu.VMEM((n_z, pair, units), bf16),
            blocks, blocks, blocks, blocks, wide, block, block, block, block, block, block,
            wide,
            pltpu.VMEM((slots, width), bf16),
            pltpu.VMEM((rows, width), f32),
            dma((16 + 2 * (units // min(units, 256)),)),
            dma((n_ep,)),
            dma((n_ep,)),
            dma((n_z - 1, 4)),
            dma((n_z - 1, 4)),
            dma((n_z + 1, 6)),
            dma((n_z + 1, 6)),
            dma((n_ep,)),
            dma((n_ep,)),
            pltpu.VMEM((taken, chans), bf16),
            pltpu.VMEM((keep, chans), bf16),
            pltpu.VMEM((keep + taken, chans), f32),
            pltpu.VMEM((taken, chans), bf16),
            pltpu.VMEM((n_tp, taken, chans), bf16),
            dma((2,)),
            dma((n_tp - 1,)),
            dma((n_tp - 1,)),
        ],
        compiler_params=pltpu.CompilerParams(
            collective_id=0, has_side_effects=True, vmem_limit_bytes=56 * 1024 * 1024
        ),
        cost_estimate=pl.CostEstimate(
            flops=6 * slots * feat * units, bytes_accessed=6 * feat * units, transcendentals=0
        ),
    )(*operands)
    return (mixer_output, expert_output)


def ring_step(
    mixer_input, mixer_gain, glu_value_weight, glu_gate_weight, conv_taps, conv_bias,
    channel_gain, channel_shift, mixer_out_weight, expert_input, expert_gain, routes,
    route_logits, gate_weight, up_weight, down_weight,
):
    n_ep, n_tp = lax.axis_size("ep"), lax.axis_size("tp")
    rows, feat = expert_input.shape
    cap = 3 * rows // n_ep
    cap = -(-cap // 16) * 16
    units = gate_weight.shape[2]
    width = feat // n_tp
    n_z, peers, pair, slots = n_ep // 2, n_tp - 1, 2 * cap, n_ep * cap
    taken, chans, taps = mixer_input.shape[0], conv_taps.shape[0], conv_taps.shape[1]
    keep = -(-(taps - 1) // 16) * 16
    vmem = pl.BlockSpec(memory_space=pltpu.VMEM)
    hbm = pl.BlockSpec(memory_space=pl.ANY)
    dma = pltpu.SemaphoreType.DMA
    expert_output, mixer_output = pl.pallas_call(
        functools.partial(step_kernel, n_ep, n_tp, cap),
        out_shape=(
            jax.ShapeDtypeStruct((rows, width), bf16),
            jax.ShapeDtypeStruct((taken, mixer_out_weight.shape[1]), bf16),
        ),
        in_specs=[vmem] * 5 + [hbm] * 3 + [vmem] * 5 + [hbm] * 4,
        out_specs=(vmem, vmem),
        scratch_shapes=[
            pltpu.VMEM((feat, units), bf16),
            pltpu.VMEM((feat, units), bf16),
            pltpu.VMEM((units, feat), bf16),
            pltpu.VMEM((rows, feat), bf16),
            pltpu.VMEM((slots, width), bf16),
            pltpu.VMEM((cap, feat), bf16),
            pltpu.VMEM((slots, feat), bf16),
            pltpu.VMEM((pair, units), bf16),
            pltpu.VMEM((n_z * peers, pair, width), bf16),
            pltpu.VMEM((n_z, pair, width), bf16),
            pltpu.VMEM((n_z * peers, pair, width), bf16),
            pltpu.VMEM((n_z, pair, width), bf16),
            pltpu.VMEM((slots, width), bf16),
            dma((7,)),
            dma((n_ep,)),
            dma((n_ep,)),
            dma((n_z * peers,)),
            dma((n_z * peers,)),
            dma((n_z * peers,)),
            dma((n_z * peers,)),
            dma((n_ep,)),
            dma((n_ep,)),
            pltpu.VMEM(mixer_input.shape, bf16),
            pltpu.VMEM(glu_value_weight.shape, bf16),
            pltpu.VMEM(glu_gate_weight.shape, bf16),
            pltpu.VMEM(mixer_out_weight.shape, bf16),
            pltpu.VMEM((taken, chans), bf16),
            pltpu.VMEM((keep, chans), bf16),
            pltpu.VMEM((keep + taken, chans), f32),
            pltpu.VMEM((taken, chans), bf16),
            pltpu.VMEM((n_tp, taken, chans), bf16),
            dma((2,)),
            dma((peers,)),
            dma((peers,)),
        ],
        compiler_params=pltpu.CompilerParams(
            collective_id=0, has_side_effects=True, vmem_limit_bytes=48 * 1024 * 1024
        ),
        cost_estimate=pl.CostEstimate(
            flops=6 * slots * feat * units, bytes_accessed=6 * feat * units, transcendentals=0
        ),
    )(
        expert_input, expert_gain[None, :], routes, routes.T, route_logits,
        gate_weight, up_weight, down_weight,
        mixer_gain[None, :], conv_taps.T, conv_bias[None, :], channel_gain[None, :],
        channel_shift[None, :], mixer_input, glu_value_weight, glu_gate_weight, mixer_out_weight,
    )
    return (mixer_output, expert_output)


def solution(mesh):
    in_specs = (
        P("ep", None),
        P(),
        P("tp", None),
        P("tp", None),
        P("tp", None),
        P("tp"),
        P(),
        P(),
        P(None, "tp"),
        P("ep", None),
        P(),
        P("ep", None),
        P("ep", None),
        P("ep", None, "tp"),
        P("ep", None, "tp"),
        P("ep", "tp", None),
    )
    out_specs = (P("ep", "tp"), P("ep", "tp"))
    return jax.shard_map(
        on_device, mesh=mesh, in_specs=in_specs, out_specs=out_specs, check_vma=False
    )
```

```python
import functools

import jax
import jax.numpy as jnp
from jax import lax
from jax.experimental import pallas as pl
from jax.experimental.pallas import tpu as pltpu
from jax.sharding import PartitionSpec as P

norm_eps = 1e-06
MESH = pl.DeviceIdType.MESH
f32 = jnp.float32
bf16 = jnp.bfloat16


def step_kernel(
    n_ep, n_tp, cap,
    x_ref, gain_ref, routes_ref, routes_t_ref, logits_ref, gate_hbm, up_hbm, down_hbm,
    mix_gain_ref, taps_ref, bias_ref, chan_gain_ref, chan_shift_ref,
    mix_hbm, value_hbm, glu_gate_hbm, mix_out_hbm,
    out_ref, mix_out_ref,
    gate_w, up_w, down_w, normed, out_part, out_pair, xin, hidden, part, own_part, got, summed, ret,
    w_sem, z_send, z_recv, ag_send, ag_recv, rs_send, rs_recv, y_send, y_recv,
    mix_in, value_w, glu_gate_w, mix_out_w, gated, tail, padded, conv_own, channels,
    tail_sem, c_send, c_recv,
):
    e = lax.axis_index("ep")
    t = lax.axis_index("tp")
    n_z = n_ep // 2
    z = e // 2
    c = e % 2
    mate = e + 1 - 2 * c
    width = out_part.shape[1]
    rows, feat = x_ref.shape
    pair = 2 * cap
    slots = n_ep * cap
    peers = n_tp - 1

    weight_copies = [
        pltpu.make_async_copy(gate_hbm.at[0], gate_w, w_sem.at[0]),
        pltpu.make_async_copy(up_hbm.at[0], up_w, w_sem.at[1]),
        pltpu.make_async_copy(down_hbm.at[0], down_w, w_sem.at[2]),
    ]
    mix_copies = [
        pltpu.make_async_copy(mix_hbm, mix_in, w_sem.at[3]),
        pltpu.make_async_copy(value_hbm, value_w, w_sem.at[4]),
        pltpu.make_async_copy(glu_gate_hbm, glu_gate_w, w_sem.at[5]),
        pltpu.make_async_copy(mix_out_hbm, mix_out_w, w_sem.at[6]),
    ]
    for copy in mix_copies[:3] + weight_copies + mix_copies[3:]:
        copy.start()

    barrier = pltpu.get_barrier_semaphore()
    for o in range(1, n_ep):
        pl.semaphore_signal(barrier, inc=1, device_id=((e + o) % n_ep, t), device_id_type=MESH)
    for o in range(1, n_tp):
        pl.semaphore_signal(barrier, inc=1, device_id=(e, (t + o) % n_tp), device_id_type=MESH)

    def rows_of(index, count):
        return pl.ds(pl.multiple_of(index * count, count), count)

    def cols_of(index, count):
        return pl.ds(pl.multiple_of(index * count, count), count)

    values = x_ref[...].astype(f32)
    scale = lax.rsqrt(jnp.mean(values * values, axis=-1, keepdims=True) + norm_eps)
    normed[...] = (values * scale * gain_ref[...]).astype(bf16)

    lanes = lax.broadcasted_iota(jnp.int32, (rows, 128), 1)
    m0 = (lanes == routes_ref[:, 0:1]).astype(f32)
    m1 = (lanes == routes_ref[:, 1:2]).astype(f32)
    ri = lax.broadcasted_iota(jnp.int32, (rows, rows), 0)
    ci = lax.broadcasted_iota(jnp.int32, (rows, rows), 1)
    lower = (ci < ri).astype(f32).astype(bf16)
    upper = (ri < ci).astype(f32).astype(bf16)
    count = jnp.dot(lower, (m0 + m1).astype(bf16), preferred_element_type=f32)
    base = count + (lanes * cap).astype(f32)
    place0 = jnp.sum(base * m0, axis=1, keepdims=True).astype(jnp.int32)
    place1 = jnp.sum(base * m1, axis=1, keepdims=True).astype(jnp.int32)
    subs = lax.broadcasted_iota(jnp.int32, (128, rows), 0)
    t0 = (subs == routes_t_ref[0:1, :]).astype(f32)
    t1 = (subs == routes_t_ref[1:2, :]).astype(f32)
    count_t = jnp.dot((t0 + t1).astype(bf16), upper, preferred_element_type=f32)
    base_t = count_t + (subs * cap).astype(f32)
    row0 = jnp.sum(base_t * t0, axis=0, keepdims=True).astype(jnp.int32)
    row1 = jnp.sum(base_t * t1, axis=0, keepdims=True).astype(jnp.int32)

    def pick(first, size):
        at = lax.broadcasted_iota(jnp.int32, (size, rows), 0) + first
        return ((at == row0) | (at == row1)).astype(f32).astype(bf16)

    out_part[...] = jnp.dot(
        pick(0, slots), normed[:, cols_of(t, width)], preferred_element_type=f32
    ).astype(bf16)

    pl.semaphore_wait(barrier, n_ep - 1 + peers)

    z_copies = []
    for k in range(1, n_z):
        for cc in range(2):
            dest = ((z + k) % n_z) * 2 + cc
            copy = pltpu.make_async_remote_copy(
                src_ref=out_part.at[rows_of(dest, cap), :],
                dst_ref=xin.at[rows_of(e, cap), cols_of(t, width)],
                send_sem=z_send.at[2 * k + cc],
                recv_sem=z_recv.at[2 * k + c],
                device_id=(dest, t),
                device_id_type=MESH,
            )
            copy.start()
            z_copies.append(copy)

    out_pair[...] = jnp.dot(
        pick(mate * cap, cap), normed[...], preferred_element_type=f32
    ).astype(bf16)
    mate_copy = pltpu.make_async_remote_copy(
        src_ref=out_pair,
        dst_ref=xin.at[rows_of(e, cap), :],
        send_sem=z_send.at[0],
        recv_sem=z_recv.at[0],
        device_id=(mate, t),
        device_id_type=MESH,
    )
    mate_copy.start()
    xin[rows_of(e, cap), :] = jnp.dot(
        pick(e * cap, cap), normed[...], preferred_element_type=f32
    ).astype(bf16)

    def source_chip(k):
        return (z + n_z - k) % n_z

    ag_copies = []

    def gather(k):
        chip = source_chip(k)
        for cc in range(2):
            block = xin.at[rows_of(chip * 2 + cc, cap), cols_of(t, width)]
            pltpu.make_async_remote_copy(
                src_ref=block, dst_ref=block, send_sem=z_send.at[2 * k + cc],
                recv_sem=z_recv.at[2 * k + cc], device_id=(mate, t), device_id_type=MESH,
            ).wait_recv()
        block = xin.at[rows_of(chip, pair), cols_of(t, width)]
        for o in range(1, n_tp):
            copy = pltpu.make_async_remote_copy(
                src_ref=block, dst_ref=block, send_sem=ag_send.at[k * peers + o - 1],
                recv_sem=ag_recv.at[k * peers + o - 1],
                device_id=(e, (t + o) % n_tp), device_id_type=MESH,
            )
            copy.start()
            ag_copies.append(copy)

    def gathered(k):
        chip = source_chip(k)
        for o in range(1, n_tp):
            block = xin.at[rows_of(chip, pair), cols_of((t + n_tp - o) % n_tp, width)]
            pltpu.make_async_remote_copy(
                src_ref=block, dst_ref=block, send_sem=ag_send.at[k * peers + o - 1],
                recv_sem=ag_recv.at[k * peers + o - 1],
                device_id=(mate, t), device_id_type=MESH,
            ).wait_recv()

    units = gate_w.shape[1]
    tile = min(units, 256)
    rs_copies = []
    y_copies = []

    def up_half(k):
        here = rows_of(source_chip(k), pair)

        def one(j, carry):
            cols = cols_of(j, tile)
            rows_in = xin[here, :]
            g = jnp.dot(rows_in, gate_w[:, cols], preferred_element_type=f32)
            u = jnp.dot(rows_in, up_w[:, cols], preferred_element_type=f32)
            hidden[:, cols] = (g * jax.nn.sigmoid(g) * u).astype(bf16)
            return carry

        lax.fori_loop(0, units // tile, one, 0)

    def down_half(k):
        for o in range(1, n_tp):
            peer = (t + o) % n_tp
            at = k * peers + o - 1
            part[at] = jnp.dot(
                hidden[...], down_w[:, cols_of(peer, width)], preferred_element_type=f32
            ).astype(bf16)
            copy = pltpu.make_async_remote_copy(
                src_ref=part.at[at], dst_ref=got.at[at], send_sem=rs_send.at[at],
                recv_sem=rs_recv.at[at], device_id=(e, peer), device_id_type=MESH,
            )
            copy.start()
            rs_copies.append(copy)
        own_part[k] = jnp.dot(
            hidden[...], down_w[:, cols_of(t, width)], preferred_element_type=f32
        ).astype(bf16)

    def finish(k):
        chip = source_chip(k)
        total = own_part[k].astype(f32)
        for o in range(1, n_tp):
            at = k * peers + o - 1
            pltpu.make_async_remote_copy(
                src_ref=part.at[at], dst_ref=got.at[at], send_sem=rs_send.at[at],
                recv_sem=rs_recv.at[at], device_id=(mate, t), device_id_type=MESH,
            ).wait_recv()
            total = total + got[at].astype(f32)
        summed[k] = total.astype(bf16)
        if k == 0:
            copy = pltpu.make_async_remote_copy(
                src_ref=summed.at[0, rows_of(1 - c, cap), :], dst_ref=ret.at[rows_of(e, cap), :],
                send_sem=y_send.at[0], recv_sem=y_recv.at[0],
                device_id=(mate, t), device_id_type=MESH,
            )
            copy.start()
            y_copies.append(copy)
            ret[rows_of(e, cap), :] = summed[0, rows_of(c, cap), :]
            return
        for cc in range(2):
            copy = pltpu.make_async_remote_copy(
                src_ref=summed.at[k, pl.ds(cc * cap, cap), :], dst_ref=ret.at[rows_of(e, cap), :],
                send_sem=y_send.at[2 * k + cc], recv_sem=y_recv.at[2 * k + c],
                device_id=(chip * 2 + cc, t), device_id_type=MESH,
            )
            copy.start()
            y_copies.append(copy)

    taken, chans = gated.shape
    keep = tail.shape[0]
    reach = taps_ref.shape[0] - 1
    conv_copies = []

    def tail_copy():
        return pltpu.make_async_remote_copy(
            src_ref=gated.at[pl.ds(taken - keep, keep), :], dst_ref=tail,
            send_sem=tail_sem.at[0], recv_sem=tail_sem.at[1],
            device_id=((e + 1) % n_ep, t), device_id_type=MESH,
        )

    def glu():
        for copy in mix_copies[:3]:
            copy.wait()
        mixed = mix_in[...].astype(f32)
        inv = lax.rsqrt(jnp.mean(mixed * mixed, axis=-1, keepdims=True) + norm_eps)
        normed_a = (mixed * inv * mix_gain_ref[...]).astype(bf16)
        contract = (((1,), (1,)), ((), ()))
        value = lax.dot_general(normed_a, value_w[...], contract, preferred_element_type=f32)
        gate = lax.dot_general(normed_a, glu_gate_w[...], contract, preferred_element_type=f32)
        gated[...] = (value * jax.nn.sigmoid(gate)).astype(bf16)
        copy = tail_copy()
        copy.start()
        conv_copies.append(copy)

    def convolve():
        tail_copy().wait_recv()
        before = tail[...].astype(f32)
        padded[pl.ds(0, keep), :] = jnp.where(e > 0, before, jnp.zeros_like(before))
        padded[pl.ds(keep, taken), :] = gated[...].astype(f32)
        total = jnp.zeros((taken, chans), f32)
        for offset in range(reach + 1):
            shift = keep - reach + offset
            total = total + padded[pl.ds(shift, taken), :] * taps_ref[offset : offset + 1, :]
        done = (total + bias_ref[...]).astype(bf16)
        conv_own[...] = done
        channels[t] = done
        for o in range(1, n_tp):
            copy = pltpu.make_async_remote_copy(
                src_ref=conv_own, dst_ref=channels.at[t],
                send_sem=c_send.at[o - 1], recv_sem=c_recv.at[o - 1],
                device_id=(e, (t + o) % n_tp), device_id_type=MESH,
            )
            copy.start()
            conv_copies.append(copy)

    def mixer_end():
        for o in range(1, n_tp):
            pltpu.make_async_remote_copy(
                src_ref=conv_own, dst_ref=channels.at[(t + n_tp - o) % n_tp],
                send_sem=c_send.at[o - 1], recv_sem=c_recv.at[o - 1],
                device_id=(mate, t), device_id_type=MESH,
            ).wait_recv()
        mix_copies[3].wait()
        chan_values = jnp.concatenate([channels[i].astype(f32) for i in range(n_tp)], axis=1)
        centered = chan_values - jnp.mean(chan_values, axis=1, keepdims=True)
        variance = jnp.mean(centered * centered, axis=1, keepdims=True)
        shaped = (
            centered * lax.rsqrt(variance + norm_eps) * chan_gain_ref[...] + chan_shift_ref[...]
        )
        activated = (shaped * jax.nn.sigmoid(shaped)).astype(bf16)
        mix_out_ref[...] = jnp.dot(
            activated, mix_out_w[...], preferred_element_type=f32
        ).astype(bf16)

    glu()
    if n_z > 1:
        gather(1)
    mate_block = xin.at[rows_of(mate, cap), :]
    pltpu.make_async_remote_copy(
        src_ref=mate_block, dst_ref=mate_block, send_sem=z_send.at[0], recv_sem=z_recv.at[0],
        device_id=(mate, t), device_id_type=MESH,
    ).wait_recv()
    weight_copies[0].wait()
    weight_copies[1].wait()
    for k in range(n_z):
        if k > 0:
            gathered(k)
        up_half(k)
        if k == 0:
            weight_copies[2].wait()
        if k + 2 < n_z:
            gather(k + 2)
        down_half(k)
        if k == 0:
            convolve()
        if k > 0:
            finish(k - 1)
        if k == 1 or n_z == 1:
            mixer_end()
    finish(n_z - 1)

    block = ret.at[rows_of(mate, cap), :]
    pltpu.make_async_remote_copy(
        src_ref=block, dst_ref=block, send_sem=y_send.at[0], recv_sem=y_recv.at[0],
        device_id=(mate, t), device_id_type=MESH,
    ).wait_recv()
    for k in range(1, n_z):
        for cc in range(2):
            block = ret.at[rows_of(((z + k) % n_z) * 2 + cc, cap), :]
            pltpu.make_async_remote_copy(
                src_ref=block, dst_ref=block, send_sem=y_send.at[2 * k + cc],
                recv_sem=y_recv.at[2 * k + cc], device_id=(mate, t), device_id_type=MESH,
            ).wait_recv()
    at = lax.broadcasted_iota(jnp.int32, (rows, slots), 1)
    l0 = logits_ref[:, 0:1]
    l1 = logits_ref[:, 1:2]
    first = jnp.dot(
        (at == place0).astype(f32).astype(bf16), ret[...], preferred_element_type=f32
    )
    second = jnp.dot(
        (at == place1).astype(f32).astype(bf16), ret[...], preferred_element_type=f32
    )
    out_ref[...] = (
        first * jax.nn.sigmoid(l0 - l1) + second * jax.nn.sigmoid(l1 - l0)
    ).astype(bf16)
    for copy in [mate_copy] + z_copies + ag_copies + rs_copies + y_copies + conv_copies:
        copy.wait_send()


outer_plan = (
    "pass0", "route2", "relay2", "route3", "join2", "up2", "more2", "far2", "relay3", "conv",
    "route1", "near2", "own2", "pass2", "up1", "more1", "far1", "join3", "up3", "more3", "far3",
    "spread", "sum2", "sum0", "near3", "pass3", "near1", "own3", "mix", "back0", "sum3", "pass1",
    "own1", "sum1", "back2", "back3", "back1",
)
inner_plan = (
    "pass0", "route2", "relay2", "route3", "join2", "up2", "more2", "far2", "relay3", "conv",
    "near2", "pass2", "join3", "up3", "more3", "far3", "own2", "near3", "sum2", "route1", "spread",
    "up1", "pass3", "more1", "far1", "own3", "near1", "mix", "pass1", "sum0", "back2", "back0",
    "own1", "sum3", "sum1", "back3", "back1",
)


def paired_kernel(
    n_ep, n_tp, cap,
    x_hbm, gain_hbm, routes_hbm, logits_hbm, gate_hbm, up_hbm, down_hbm,
    mix_gain_hbm, taps_hbm, bias_hbm, chan_gain_hbm, chan_shift_hbm,
    mix_hbm, value_hbm, glu_gate_hbm, mix_out_hbm,
    out_ref, mix_out_ref,
    x_in, gain_in, routes_in, logits_in, gate_w, up_w, down_w,
    mix_gain_in, taps_in, bias_in, chan_gain_in, chan_shift_in,
    mix_in, value_w, glu_gate_w, mix_out_w,
    normed, columns, out_part, out_pair, out_near, xin, hidden,
    part_x, part_y, got_x, got_y, held_own, held_x, held_y, pass_x, pass_y, last_x, last_y,
    summed, ret, acc,
    load_sem, z_send, z_recv, ag_send, ag_recv, rs_send, rs_recv, y_send, y_recv,
    gated, tail, padded, conv_own, channels,
    tail_sem, c_send, c_recv,
):
    e = lax.axis_index("ep")
    t = lax.axis_index("tp")
    n_z = n_ep // 2
    z = e // 2
    c = e % 2
    mate = e + 1 - 2 * c
    rows, feat = x_in.shape
    width = out_part.shape[2]
    half = width // 2
    pair = 2 * cap
    slots = n_ep * cap
    units = gate_w.shape[1]
    tile = min(units, 256)
    tiles = units // tile
    t_x = t + 1 - 2 * (t % 2)
    t_y = (t + 2) % 4
    t_d = 3 - t

    def chip_of(k):
        return [z, z + 1 - 2 * (z % 2), (z + 2) % 4, 3 - z][k]

    inner = (z + 1) // 2 % 2

    def rows_of(index, count):
        return pl.ds(pl.multiple_of(index * count, count), count)

    def cols(quarter, first, count):
        return pl.ds(pl.multiple_of(quarter * width + first, 128), count)

    def load(src, dst, at):
        return pltpu.make_async_copy(src, dst, load_sem.at[at])

    def weight_tile(j):
        here = pl.ds(pl.multiple_of(j * tile, tile), tile)
        return (
            load(gate_hbm.at[0, :, here], gate_w.at[:, here], 16 + 2 * j),
            load(up_hbm.at[0, :, here], up_w.at[:, here], 17 + 2 * j),
        )

    load_routes = load(routes_hbm, routes_in, 0)
    load_logits = load(logits_hbm, logits_in, 1)
    load_gain = load(gain_hbm, gain_in, 2)
    load_x = load(x_hbm, x_in, 3)
    load_mix = [
        load(mix_hbm, mix_in, 4), load(mix_gain_hbm, mix_gain_in, 5),
        load(value_hbm, value_w, 6), load(glu_gate_hbm, glu_gate_w, 7),
    ]
    load_conv = [load(taps_hbm, taps_in, 8), load(bias_hbm, bias_in, 9)]
    load_end = [
        load(chan_gain_hbm, chan_gain_in, 10), load(chan_shift_hbm, chan_shift_in, 11),
        load(mix_out_hbm, mix_out_w, 12),
    ]
    load_down = load(down_hbm.at[0], down_w, 13)
    for copy in [load_x, load_gain, load_routes, load_logits] + load_mix + load_conv:
        copy.start()
    for j in range(tiles):
        for copy in weight_tile(j):
            copy.start()
    for copy in [load_down] + load_end:
        copy.start()

    barrier = pltpu.get_barrier_semaphore()
    for o in range(1, n_ep):
        pl.semaphore_signal(barrier, inc=1, device_id=((e + o) % n_ep, t), device_id_type=MESH)
    for o in range(1, n_tp):
        pl.semaphore_signal(barrier, inc=1, device_id=(e, (t + o) % n_tp), device_id_type=MESH)

    load_routes.wait()
    ri = lax.broadcasted_iota(jnp.int32, (rows, rows), 0)
    ci = lax.broadcasted_iota(jnp.int32, (rows, rows), 1)
    upper = (ri < ci).astype(f32).astype(bf16)
    subs = lax.broadcasted_iota(jnp.int32, (128, rows), 0)
    t0 = (subs == routes_in[0:1, :]).astype(f32)
    t1 = (subs == routes_in[1:2, :]).astype(f32)
    count_t = jnp.dot((t0 + t1).astype(bf16), upper, preferred_element_type=f32)
    base_t = count_t + (subs * cap).astype(f32)
    place0 = jnp.sum(base_t * t0, axis=0, keepdims=True)
    place1 = jnp.sum(base_t * t1, axis=0, keepdims=True)
    row0 = place0.astype(jnp.int32)
    row1 = place1.astype(jnp.int32)

    def pick(first, size):
        at = lax.broadcasted_iota(jnp.int32, (size, rows), 0) + first
        return ((at == row0) | (at == row1)).astype(f32).astype(bf16)

    load_x.wait()
    load_gain.wait()
    values = x_in[...].astype(f32)
    scale = lax.rsqrt(jnp.mean(values * values, axis=-1, keepdims=True) + norm_eps)
    normed[...] = (values * scale * gain_in[...]).astype(bf16)
    for k in (2, 3):
        out_part[k - 2] = jnp.dot(
            pick(chip_of(k) * pair, pair), normed[:, cols(t, 0, width)],
            preferred_element_type=f32,
        ).astype(bf16)

    pl.semaphore_wait(barrier, n_ep - 1 + n_tp - 1)

    sent = []

    def send(src, dst, send_sem, recv_sem, to):
        copy = pltpu.make_async_remote_copy(
            src_ref=src, dst_ref=dst, send_sem=send_sem, recv_sem=recv_sem,
            device_id=to, device_id_type=MESH,
        )
        copy.start()
        sent.append(copy)

    def arrive(dst, send_sem, recv_sem):
        pltpu.make_async_remote_copy(
            src_ref=dst, dst_ref=dst, send_sem=send_sem, recv_sem=recv_sem,
            device_id=(mate, t), device_id_type=MESH,
        ).wait_recv()

    for k in (2, 3):
        for cc in range(2):
            dest = chip_of(k) * 2 + cc
            send(
                out_part.at[k - 2, pl.ds(cc * cap, cap), :],
                xin.at[rows_of(e, cap), cols(t, 0, width)],
                z_send.at[2 * k + cc], z_recv.at[2 * k + c], (dest, t),
            )

    out_pair[...] = jnp.dot(
        pick(mate * cap, cap), normed[...], preferred_element_type=f32
    ).astype(bf16)
    send(out_pair, xin.at[rows_of(e, cap), :], z_send.at[0], z_recv.at[0], (mate, t))
    for cc in range(2):
        dest = chip_of(1) * 2 + cc
        out_near[cc] = jnp.dot(
            pick(dest * cap, cap), normed[...], preferred_element_type=f32
        ).astype(bf16)
        send(
            out_near.at[cc], xin.at[rows_of(e, cap), :],
            z_send.at[2 + cc], z_recv.at[2 + c], (dest, t),
        )
    xin[rows_of(e, cap), :] = jnp.dot(
        pick(e * cap, cap), normed[...], preferred_element_type=f32
    ).astype(bf16)

    def routed(k):
        for cc in range(2):
            here = rows_of(chip_of(k) * 2 + cc, cap)
            arrive(
                xin.at[here, :] if k == 1 else xin.at[here, cols(t, 0, width)],
                z_send.at[2 * k + cc], z_recv.at[2 * k + cc],
            )
        if k == 1:
            return
        block = xin.at[rows_of(chip_of(k), pair), cols(t, 0, width)]
        send(block, block, ag_send.at[k - 2, 0], ag_recv.at[k - 2, 0], (e, t_x))
        send(block, block, ag_send.at[k - 2, 1], ag_recv.at[k - 2, 1], (e, t_y))

    def relay(k):
        here = rows_of(chip_of(k), pair)
        arrive(xin.at[here, cols(t_y, 0, width)], ag_send.at[k - 2, 1], ag_recv.at[k - 2, 1])
        block = xin.at[here, cols(t_y, 0, half)]
        send(block, block, ag_send.at[k - 2, 2], ag_recv.at[k - 2, 2], (e, t_x))
        arrive(xin.at[here, cols(t_x, 0, width)], ag_send.at[k - 2, 0], ag_recv.at[k - 2, 0])
        block = xin.at[here, cols(t_x, half, half)]
        send(block, block, ag_send.at[k - 2, 3], ag_recv.at[k - 2, 3], (e, t_y))

    def gathered(k):
        here = rows_of(chip_of(k), pair)
        arrive(xin.at[here, cols(t_d, 0, half)], ag_send.at[k - 2, 2], ag_recv.at[k - 2, 2])
        arrive(xin.at[here, cols(t_d, half, half)], ag_send.at[k - 2, 3], ag_recv.at[k - 2, 3])

    def up_half(k, first, last):
        here = rows_of(chip_of(k), pair)

        def one(j, carry):
            if k == 0:
                for copy in weight_tile(j):
                    copy.wait()
            at = pl.ds(pl.multiple_of(j * tile, tile), tile)
            rows_in = xin[here, :]
            g = jnp.dot(rows_in, gate_w[:, at], preferred_element_type=f32)
            u = jnp.dot(rows_in, up_w[:, at], preferred_element_type=f32)
            hidden[k, :, at] = (g * jax.nn.sigmoid(g) * u).astype(bf16)
            return carry

        lax.fori_loop(first, last, one, 0)

    def product(k, quarter):
        return jnp.dot(
            hidden[k], down_w[:, cols(quarter, 0, width)], preferred_element_type=f32
        ).astype(bf16)

    def give(k, way, src, dst, to):
        send(src, dst, rs_send.at[k, way], rs_recv.at[k, way], (e, to))

    def down_far(k):
        far = product(k, t_d)
        part_x[k, 1] = far[:, :half]
        part_y[k, 1] = far[:, half:]
        give(k, 0, part_x.at[k, 1], got_x.at[k, 1], t_x)
        give(k, 1, part_y.at[k, 1], got_y.at[k, 1], t_y)

    def down_near(k):
        near = product(k, t_x)
        part_x[k, 0] = near[:, :half]
        held_x[k] = near[:, half:]
        give(k, 2, part_x.at[k, 0], got_x.at[k, 0], t_x)
        near = product(k, t_y)
        part_y[k, 0] = near[:, half:]
        held_y[k] = near[:, :half]
        give(k, 3, part_y.at[k, 0], got_y.at[k, 0], t_y)

    def down_own(k):
        held_own[k] = product(k, t)

    def pass_on(k):
        arrive(got_x.at[k, 1], rs_send.at[k, 0], rs_recv.at[k, 0])
        pass_y[k] = (held_y[k].astype(f32) + got_x[k, 1].astype(f32)).astype(bf16)
        give(k, 4, pass_y.at[k], last_y.at[k], t_y)
        arrive(got_y.at[k, 1], rs_send.at[k, 1], rs_recv.at[k, 1])
        pass_x[k] = (held_x[k].astype(f32) + got_y[k, 1].astype(f32)).astype(bf16)
        give(k, 5, pass_x.at[k], last_x.at[k], t_x)

    def finish(k):
        arrive(got_x.at[k, 0], rs_send.at[k, 2], rs_recv.at[k, 2])
        arrive(got_y.at[k, 0], rs_send.at[k, 3], rs_recv.at[k, 3])
        arrive(last_y.at[k], rs_send.at[k, 4], rs_recv.at[k, 4])
        arrive(last_x.at[k], rs_send.at[k, 5], rs_recv.at[k, 5])
        summed[k, :, :half] = (
            held_own[k, :, :half].astype(f32)
            + got_x[k, 0].astype(f32) + last_y[k].astype(f32)
        ).astype(bf16)
        summed[k, :, half:] = (
            held_own[k, :, half:].astype(f32)
            + got_y[k, 0].astype(f32) + last_x[k].astype(f32)
        ).astype(bf16)
        if k == 0:
            send(
                summed.at[0, rows_of(1 - c, cap), :], ret.at[rows_of(e, cap), :],
                y_send.at[0], y_recv.at[0], (mate, t),
            )
            ret[rows_of(e, cap), :] = summed[0, rows_of(c, cap), :]
            return
        for cc in range(2):
            send(
                summed.at[k, pl.ds(cc * cap, cap), :], ret.at[rows_of(e, cap), :],
                y_send.at[2 * k + cc], y_recv.at[2 * k + c], (chip_of(k) * 2 + cc, t),
            )

    def weighted(first, size):
        at = lax.broadcasted_iota(jnp.int32, (rows, size), 1) + first
        back = ret[rows_of(first // size, size), :]
        one = jnp.dot(
            (at == columns[0, :, 0:1].astype(jnp.int32)).astype(f32).astype(bf16), back,
            preferred_element_type=f32,
        )
        two = jnp.dot(
            (at == columns[1, :, 0:1].astype(jnp.int32)).astype(f32).astype(bf16), back,
            preferred_element_type=f32,
        )
        return one * columns[2, :, 0:1] + two * columns[3, :, 0:1]

    def returned(k):
        if k == 0:
            arrive(ret.at[rows_of(mate, cap), :], y_send.at[0], y_recv.at[0])
        for cc in range(2 if k > 0 else 0):
            arrive(
                ret.at[rows_of(chip_of(k) * 2 + cc, cap), :],
                y_send.at[2 * k + cc], y_recv.at[2 * k + cc],
            )
        return weighted(chip_of(k) * pair, pair)

    taken, chans = gated.shape
    keep = tail.shape[0]
    reach = taps_in.shape[0] - 1

    def tail_refs():
        return gated.at[pl.ds(taken - keep, keep), :], tail, tail_sem.at[0], tail_sem.at[1]

    def glu():
        for copy in load_mix:
            copy.wait()
        mixed = mix_in[...].astype(f32)
        inv = lax.rsqrt(jnp.mean(mixed * mixed, axis=-1, keepdims=True) + norm_eps)
        normed_a = (mixed * inv * mix_gain_in[...]).astype(bf16)
        contract = (((1,), (1,)), ((), ()))
        value = lax.dot_general(normed_a, value_w[...], contract, preferred_element_type=f32)
        gate = lax.dot_general(normed_a, glu_gate_w[...], contract, preferred_element_type=f32)
        gated[...] = (value * jax.nn.sigmoid(gate)).astype(bf16)
        send(*tail_refs(), ((e + 1) % n_ep, t))

    def convolve():
        for copy in load_conv:
            copy.wait()
        arrive(tail, tail_sem.at[0], tail_sem.at[1])
        before = tail[...].astype(f32)
        padded[pl.ds(0, keep), :] = jnp.where(e > 0, before, jnp.zeros_like(before))
        padded[pl.ds(keep, taken), :] = gated[...].astype(f32)
        total = jnp.zeros((taken, chans), f32)
        for offset in range(reach + 1):
            shift = keep - reach + offset
            total = total + padded[pl.ds(shift, taken), :] * taps_in[offset : offset + 1, :]
        done = (total + bias_in[...]).astype(bf16)
        conv_own[...] = done
        channels[t] = done
        for o in range(1, n_tp):
            send(
                conv_own, channels.at[t], c_send.at[o - 1], c_recv.at[o - 1],
                (e, (t + o) % n_tp),
            )

    def mixer_end():
        for o in range(1, n_tp):
            arrive(channels.at[(t + n_tp - o) % n_tp], c_send.at[o - 1], c_recv.at[o - 1])
        for copy in load_end:
            copy.wait()
        chan_values = jnp.concatenate([channels[i].astype(f32) for i in range(n_tp)], axis=1)
        centered = chan_values - jnp.mean(chan_values, axis=1, keepdims=True)
        variance = jnp.mean(centered * centered, axis=1, keepdims=True)
        shaped = (
            centered * lax.rsqrt(variance + norm_eps) * chan_gain_in[...] + chan_shift_in[...]
        )
        activated = (shaped * jax.nn.sigmoid(shaped)).astype(bf16)
        mix_out_ref[...] = jnp.dot(
            activated, mix_out_w[...], preferred_element_type=f32
        ).astype(bf16)

    def spread():
        load_logits.wait()
        columns[0] = jnp.broadcast_to(place0, (128, rows)).T
        columns[1] = jnp.broadcast_to(place1, (128, rows)).T
        lead = logits_in[0:1, :] - logits_in[1:2, :]
        columns[2] = jnp.broadcast_to(jax.nn.sigmoid(lead), (128, rows)).T
        columns[3] = jnp.broadcast_to(jax.nn.sigmoid(-lead), (128, rows)).T

    steps = {
        "route": routed, "relay": relay, "join": gathered,
        "up": lambda k: up_half(k, 0, tiles // 2), "more": lambda k: up_half(k, tiles // 2, tiles),
        "far": down_far, "near": down_near, "own": down_own,
        "pass": pass_on, "sum": finish, "spread": spread, "conv": convolve, "mix": mixer_end,
    }

    def run(plan):
        back = []
        for step in plan:
            name, at = step.rstrip("0123"), [int(step[-1])] if step[-1].isdigit() else []
            with jax.named_scope(step):
                if name != "back":
                    steps[name](*at)
                    continue
                part = returned(*at)
                back.append(step)
                if len(back) == 1:
                    acc[...] = part
                elif len(back) < n_z:
                    acc[...] += part
                else:
                    out_ref[...] = (acc[...] + part).astype(bf16)

    glu()
    arrive(xin.at[rows_of(mate, cap), :], z_send.at[0], z_recv.at[0])
    up_half(0, 0, tiles)
    load_down.wait()
    down_far(0)
    down_near(0)
    down_own(0)
    early = len(sent)
    for side, plan in ((0, outer_plan), (1, inner_plan)):

        @pl.when(inner == side)
        def one_side(plan=plan):
            run(plan)
            for copy in sent[early:]:
                copy.wait_send()
            del sent[early:]

    for copy in sent:
        copy.wait_send()


def on_device(*args):
    n_ep, n_tp = lax.axis_size("ep"), lax.axis_size("tp")
    if n_tp == 4 and n_ep == 8:
        return paired_step(*args)
    return ring_step(*args)


def paired_step(
    mixer_input, mixer_gain, glu_value_weight, glu_gate_weight, conv_taps, conv_bias,
    channel_gain, channel_shift, mixer_out_weight, expert_input, expert_gain, routes,
    route_logits, gate_weight, up_weight, down_weight,
):
    n_ep, n_tp = lax.axis_size("ep"), lax.axis_size("tp")
    rows, feat = expert_input.shape
    cap = 3 * rows // n_ep
    cap = -(-cap // 16) * 16
    units = gate_weight.shape[2]
    width = feat // n_tp
    half = width // 2
    n_z, pair, slots = n_ep // 2, 2 * cap, n_ep * cap
    taken, chans, taps = mixer_input.shape[0], conv_taps.shape[0], conv_taps.shape[1]
    keep = -(-(taps - 1) // 16) * 16
    dma = pltpu.SemaphoreType.DMA
    operands = (
        expert_input, expert_gain[None, :], routes.T, route_logits.T,
        gate_weight, up_weight, down_weight,
        mixer_gain[None, :], conv_taps.T, conv_bias[None, :], channel_gain[None, :],
        channel_shift[None, :], mixer_input, glu_value_weight, glu_gate_weight, mixer_out_weight,
    )

    def held(array):
        shape = array.shape[1:] if array.ndim == 3 else array.shape
        return pltpu.VMEM(shape, array.dtype)

    block = pltpu.VMEM((n_z, pair, half), bf16)
    blocks = pltpu.VMEM((n_z, 2, pair, half), bf16)
    wide = pltpu.VMEM((n_z, pair, width), bf16)
    vmem = pl.BlockSpec(memory_space=pltpu.VMEM)
    expert_output, mixer_output = pl.pallas_call(
        functools.partial(paired_kernel, n_ep, n_tp, cap),
        out_shape=(
            jax.ShapeDtypeStruct((rows, width), bf16),
            jax.ShapeDtypeStruct((taken, mixer_out_weight.shape[1]), bf16),
        ),
        in_specs=[pl.BlockSpec(memory_space=pltpu.HBM)] * len(operands),
        out_specs=(vmem, vmem),
        scratch_shapes=[held(array) for array in operands] + [
            pltpu.VMEM((rows, feat), bf16),
            pltpu.VMEM((4, rows, 128), f32),
            pltpu.VMEM((2, pair, width), bf16),
            pltpu.VMEM((cap, feat), bf16),
            pltpu.VMEM((2, cap, feat), bf16),
            pltpu.VMEM((slots, feat), bf16),
            pltpu.VMEM((n_z, pair, units), bf16),
            blocks, blocks, blocks, blocks, wide, block, block, block, block, block, block,
            wide,
            pltpu.VMEM((slots, width), bf16),
            pltpu.VMEM((rows, width), f32),
            dma((16 + 2 * (units // min(units, 256)),)),
            dma((n_ep,)),
            dma((n_ep,)),
            dma((n_z - 2, 4)),
            dma((n_z - 2, 4)),
            dma((n_z, 6)),
            dma((n_z, 6)),
            dma((n_ep,)),
            dma((n_ep,)),
            pltpu.VMEM((taken, chans), bf16),
            pltpu.VMEM((keep, chans), bf16),
            pltpu.VMEM((keep + taken, chans), f32),
            pltpu.VMEM((taken, chans), bf16),
            pltpu.VMEM((n_tp, taken, chans), bf16),
            dma((2,)),
            dma((n_tp - 1,)),
            dma((n_tp - 1,)),
        ],
        compiler_params=pltpu.CompilerParams(
            collective_id=0, has_side_effects=True, vmem_limit_bytes=56 * 1024 * 1024
        ),
        cost_estimate=pl.CostEstimate(
            flops=6 * slots * feat * units, bytes_accessed=6 * feat * units, transcendentals=0
        ),
    )(*operands)
    return (mixer_output, expert_output)


def ring_step(
    mixer_input, mixer_gain, glu_value_weight, glu_gate_weight, conv_taps, conv_bias,
    channel_gain, channel_shift, mixer_out_weight, expert_input, expert_gain, routes,
    route_logits, gate_weight, up_weight, down_weight,
):
    n_ep, n_tp = lax.axis_size("ep"), lax.axis_size("tp")
    rows, feat = expert_input.shape
    cap = 3 * rows // n_ep
    cap = -(-cap // 16) * 16
    units = gate_weight.shape[2]
    width = feat // n_tp
    n_z, peers, pair, slots = n_ep // 2, n_tp - 1, 2 * cap, n_ep * cap
    taken, chans, taps = mixer_input.shape[0], conv_taps.shape[0], conv_taps.shape[1]
    keep = -(-(taps - 1) // 16) * 16
    vmem = pl.BlockSpec(memory_space=pltpu.VMEM)
    hbm = pl.BlockSpec(memory_space=pl.ANY)
    dma = pltpu.SemaphoreType.DMA
    expert_output, mixer_output = pl.pallas_call(
        functools.partial(step_kernel, n_ep, n_tp, cap),
        out_shape=(
            jax.ShapeDtypeStruct((rows, width), bf16),
            jax.ShapeDtypeStruct((taken, mixer_out_weight.shape[1]), bf16),
        ),
        in_specs=[vmem] * 5 + [hbm] * 3 + [vmem] * 5 + [hbm] * 4,
        out_specs=(vmem, vmem),
        scratch_shapes=[
            pltpu.VMEM((feat, units), bf16),
            pltpu.VMEM((feat, units), bf16),
            pltpu.VMEM((units, feat), bf16),
            pltpu.VMEM((rows, feat), bf16),
            pltpu.VMEM((slots, width), bf16),
            pltpu.VMEM((cap, feat), bf16),
            pltpu.VMEM((slots, feat), bf16),
            pltpu.VMEM((pair, units), bf16),
            pltpu.VMEM((n_z * peers, pair, width), bf16),
            pltpu.VMEM((n_z, pair, width), bf16),
            pltpu.VMEM((n_z * peers, pair, width), bf16),
            pltpu.VMEM((n_z, pair, width), bf16),
            pltpu.VMEM((slots, width), bf16),
            dma((7,)),
            dma((n_ep,)),
            dma((n_ep,)),
            dma((n_z * peers,)),
            dma((n_z * peers,)),
            dma((n_z * peers,)),
            dma((n_z * peers,)),
            dma((n_ep,)),
            dma((n_ep,)),
            pltpu.VMEM(mixer_input.shape, bf16),
            pltpu.VMEM(glu_value_weight.shape, bf16),
            pltpu.VMEM(glu_gate_weight.shape, bf16),
            pltpu.VMEM(mixer_out_weight.shape, bf16),
            pltpu.VMEM((taken, chans), bf16),
            pltpu.VMEM((keep, chans), bf16),
            pltpu.VMEM((keep + taken, chans), f32),
            pltpu.VMEM((taken, chans), bf16),
            pltpu.VMEM((n_tp, taken, chans), bf16),
            dma((2,)),
            dma((peers,)),
            dma((peers,)),
        ],
        compiler_params=pltpu.CompilerParams(
            collective_id=0, has_side_effects=True, vmem_limit_bytes=48 * 1024 * 1024
        ),
        cost_estimate=pl.CostEstimate(
            flops=6 * slots * feat * units, bytes_accessed=6 * feat * units, transcendentals=0
        ),
    )(
        expert_input, expert_gain[None, :], routes, routes.T, route_logits,
        gate_weight, up_weight, down_weight,
        mixer_gain[None, :], conv_taps.T, conv_bias[None, :], channel_gain[None, :],
        channel_shift[None, :], mixer_input, glu_value_weight, glu_gate_weight, mixer_out_weight,
    )
    return (mixer_output, expert_output)


def solution(mesh):
    in_specs = (
        P("ep", None),
        P(),
        P("tp", None),
        P("tp", None),
        P("tp", None),
        P("tp"),
        P(),
        P(),
        P(None, "tp"),
        P("ep", None),
        P(),
        P("ep", None),
        P("ep", None),
        P("ep", None, "tp"),
        P("ep", None, "tp"),
        P("ep", "tp", None),
    )
    out_specs = (P("ep", "tp"), P("ep", "tp"))
    return jax.shard_map(
        on_device, mesh=mesh, in_specs=in_specs, out_specs=out_specs, check_vma=False
    )
```

```python
import functools

import jax
import jax.numpy as jnp
from jax import lax
from jax.experimental import pallas as pl
from jax.experimental.pallas import tpu as pltpu
from jax.sharding import PartitionSpec as P

norm_eps = 1e-06
MESH = pl.DeviceIdType.MESH
f32 = jnp.float32
bf16 = jnp.bfloat16


def step_kernel(
    n_ep, n_tp, cap,
    x_ref, gain_ref, routes_ref, routes_t_ref, logits_ref, gate_hbm, up_hbm, down_hbm,
    mix_gain_ref, taps_ref, bias_ref, chan_gain_ref, chan_shift_ref,
    mix_hbm, value_hbm, glu_gate_hbm, mix_out_hbm,
    out_ref, mix_out_ref,
    gate_w, up_w, down_w, normed, out_part, out_pair, xin, hidden, part, own_part, got, summed, ret,
    w_sem, z_send, z_recv, ag_send, ag_recv, rs_send, rs_recv, y_send, y_recv,
    mix_in, value_w, glu_gate_w, mix_out_w, gated, tail, padded, conv_own, channels,
    tail_sem, c_send, c_recv,
):
    e = lax.axis_index("ep")
    t = lax.axis_index("tp")
    n_z = n_ep // 2
    z = e // 2
    c = e % 2
    mate = e + 1 - 2 * c
    width = out_part.shape[1]
    rows, feat = x_ref.shape
    pair = 2 * cap
    slots = n_ep * cap
    peers = n_tp - 1

    weight_copies = [
        pltpu.make_async_copy(gate_hbm.at[0], gate_w, w_sem.at[0]),
        pltpu.make_async_copy(up_hbm.at[0], up_w, w_sem.at[1]),
        pltpu.make_async_copy(down_hbm.at[0], down_w, w_sem.at[2]),
    ]
    mix_copies = [
        pltpu.make_async_copy(mix_hbm, mix_in, w_sem.at[3]),
        pltpu.make_async_copy(value_hbm, value_w, w_sem.at[4]),
        pltpu.make_async_copy(glu_gate_hbm, glu_gate_w, w_sem.at[5]),
        pltpu.make_async_copy(mix_out_hbm, mix_out_w, w_sem.at[6]),
    ]
    for copy in mix_copies[:3] + weight_copies + mix_copies[3:]:
        copy.start()

    barrier = pltpu.get_barrier_semaphore()
    for o in range(1, n_ep):
        pl.semaphore_signal(barrier, inc=1, device_id=((e + o) % n_ep, t), device_id_type=MESH)
    for o in range(1, n_tp):
        pl.semaphore_signal(barrier, inc=1, device_id=(e, (t + o) % n_tp), device_id_type=MESH)

    def rows_of(index, count):
        return pl.ds(pl.multiple_of(index * count, count), count)

    def cols_of(index, count):
        return pl.ds(pl.multiple_of(index * count, count), count)

    values = x_ref[...].astype(f32)
    scale = lax.rsqrt(jnp.mean(values * values, axis=-1, keepdims=True) + norm_eps)
    normed[...] = (values * scale * gain_ref[...]).astype(bf16)

    lanes = lax.broadcasted_iota(jnp.int32, (rows, 128), 1)
    m0 = (lanes == routes_ref[:, 0:1]).astype(f32)
    m1 = (lanes == routes_ref[:, 1:2]).astype(f32)
    ri = lax.broadcasted_iota(jnp.int32, (rows, rows), 0)
    ci = lax.broadcasted_iota(jnp.int32, (rows, rows), 1)
    lower = (ci < ri).astype(f32).astype(bf16)
    upper = (ri < ci).astype(f32).astype(bf16)
    count = jnp.dot(lower, (m0 + m1).astype(bf16), preferred_element_type=f32)
    base = count + (lanes * cap).astype(f32)
    place0 = jnp.sum(base * m0, axis=1, keepdims=True).astype(jnp.int32)
    place1 = jnp.sum(base * m1, axis=1, keepdims=True).astype(jnp.int32)
    subs = lax.broadcasted_iota(jnp.int32, (128, rows), 0)
    t0 = (subs == routes_t_ref[0:1, :]).astype(f32)
    t1 = (subs == routes_t_ref[1:2, :]).astype(f32)
    count_t = jnp.dot((t0 + t1).astype(bf16), upper, preferred_element_type=f32)
    base_t = count_t + (subs * cap).astype(f32)
    row0 = jnp.sum(base_t * t0, axis=0, keepdims=True).astype(jnp.int32)
    row1 = jnp.sum(base_t * t1, axis=0, keepdims=True).astype(jnp.int32)

    def pick(first, size):
        at = lax.broadcasted_iota(jnp.int32, (size, rows), 0) + first
        return ((at == row0) | (at == row1)).astype(f32).astype(bf16)

    out_part[...] = jnp.dot(
        pick(0, slots), normed[:, cols_of(t, width)], preferred_element_type=f32
    ).astype(bf16)

    pl.semaphore_wait(barrier, n_ep - 1 + peers)

    z_copies = []
    for k in range(1, n_z):
        for cc in range(2):
            dest = ((z + k) % n_z) * 2 + cc
            copy = pltpu.make_async_remote_copy(
                src_ref=out_part.at[rows_of(dest, cap), :],
                dst_ref=xin.at[rows_of(e, cap), cols_of(t, width)],
                send_sem=z_send.at[2 * k + cc],
                recv_sem=z_recv.at[2 * k + c],
                device_id=(dest, t),
                device_id_type=MESH,
            )
            copy.start()
            z_copies.append(copy)

    out_pair[...] = jnp.dot(
        pick(mate * cap, cap), normed[...], preferred_element_type=f32
    ).astype(bf16)
    mate_copy = pltpu.make_async_remote_copy(
        src_ref=out_pair,
        dst_ref=xin.at[rows_of(e, cap), :],
        send_sem=z_send.at[0],
        recv_sem=z_recv.at[0],
        device_id=(mate, t),
        device_id_type=MESH,
    )
    mate_copy.start()
    xin[rows_of(e, cap), :] = jnp.dot(
        pick(e * cap, cap), normed[...], preferred_element_type=f32
    ).astype(bf16)

    def source_chip(k):
        return (z + n_z - k) % n_z

    ag_copies = []

    def gather(k):
        chip = source_chip(k)
        for cc in range(2):
            block = xin.at[rows_of(chip * 2 + cc, cap), cols_of(t, width)]
            pltpu.make_async_remote_copy(
                src_ref=block, dst_ref=block, send_sem=z_send.at[2 * k + cc],
                recv_sem=z_recv.at[2 * k + cc], device_id=(mate, t), device_id_type=MESH,
            ).wait_recv()
        block = xin.at[rows_of(chip, pair), cols_of(t, width)]
        for o in range(1, n_tp):
            copy = pltpu.make_async_remote_copy(
                src_ref=block, dst_ref=block, send_sem=ag_send.at[k * peers + o - 1],
                recv_sem=ag_recv.at[k * peers + o - 1],
                device_id=(e, (t + o) % n_tp), device_id_type=MESH,
            )
            copy.start()
            ag_copies.append(copy)

    def gathered(k):
        chip = source_chip(k)
        for o in range(1, n_tp):
            block = xin.at[rows_of(chip, pair), cols_of((t + n_tp - o) % n_tp, width)]
            pltpu.make_async_remote_copy(
                src_ref=block, dst_ref=block, send_sem=ag_send.at[k * peers + o - 1],
                recv_sem=ag_recv.at[k * peers + o - 1],
                device_id=(mate, t), device_id_type=MESH,
            ).wait_recv()

    units = gate_w.shape[1]
    tile = min(units, 256)
    rs_copies = []
    y_copies = []

    def up_half(k):
        here = rows_of(source_chip(k), pair)

        def one(j, carry):
            cols = cols_of(j, tile)
            rows_in = xin[here, :]
            g = jnp.dot(rows_in, gate_w[:, cols], preferred_element_type=f32)
            u = jnp.dot(rows_in, up_w[:, cols], preferred_element_type=f32)
            hidden[:, cols] = (g * jax.nn.sigmoid(g) * u).astype(bf16)
            return carry

        lax.fori_loop(0, units // tile, one, 0)

    def down_half(k):
        for o in range(1, n_tp):
            peer = (t + o) % n_tp
            at = k * peers + o - 1
            part[at] = jnp.dot(
                hidden[...], down_w[:, cols_of(peer, width)], preferred_element_type=f32
            ).astype(bf16)
            copy = pltpu.make_async_remote_copy(
                src_ref=part.at[at], dst_ref=got.at[at], send_sem=rs_send.at[at],
                recv_sem=rs_recv.at[at], device_id=(e, peer), device_id_type=MESH,
            )
            copy.start()
            rs_copies.append(copy)
        own_part[k] = jnp.dot(
            hidden[...], down_w[:, cols_of(t, width)], preferred_element_type=f32
        ).astype(bf16)

    def finish(k):
        chip = source_chip(k)
        total = own_part[k].astype(f32)
        for o in range(1, n_tp):
            at = k * peers + o - 1
            pltpu.make_async_remote_copy(
                src_ref=part.at[at], dst_ref=got.at[at], send_sem=rs_send.at[at],
                recv_sem=rs_recv.at[at], device_id=(mate, t), device_id_type=MESH,
            ).wait_recv()
            total = total + got[at].astype(f32)
        summed[k] = total.astype(bf16)
        if k == 0:
            copy = pltpu.make_async_remote_copy(
                src_ref=summed.at[0, rows_of(1 - c, cap), :], dst_ref=ret.at[rows_of(e, cap), :],
                send_sem=y_send.at[0], recv_sem=y_recv.at[0],
                device_id=(mate, t), device_id_type=MESH,
            )
            copy.start()
            y_copies.append(copy)
            ret[rows_of(e, cap), :] = summed[0, rows_of(c, cap), :]
            return
        for cc in range(2):
            copy = pltpu.make_async_remote_copy(
                src_ref=summed.at[k, pl.ds(cc * cap, cap), :], dst_ref=ret.at[rows_of(e, cap), :],
                send_sem=y_send.at[2 * k + cc], recv_sem=y_recv.at[2 * k + c],
                device_id=(chip * 2 + cc, t), device_id_type=MESH,
            )
            copy.start()
            y_copies.append(copy)

    taken, chans = gated.shape
    keep = tail.shape[0]
    reach = taps_ref.shape[0] - 1
    conv_copies = []

    def tail_copy():
        return pltpu.make_async_remote_copy(
            src_ref=gated.at[pl.ds(taken - keep, keep), :], dst_ref=tail,
            send_sem=tail_sem.at[0], recv_sem=tail_sem.at[1],
            device_id=((e + 1) % n_ep, t), device_id_type=MESH,
        )

    def glu():
        for copy in mix_copies[:3]:
            copy.wait()
        mixed = mix_in[...].astype(f32)
        inv = lax.rsqrt(jnp.mean(mixed * mixed, axis=-1, keepdims=True) + norm_eps)
        normed_a = (mixed * inv * mix_gain_ref[...]).astype(bf16)
        contract = (((1,), (1,)), ((), ()))
        value = lax.dot_general(normed_a, value_w[...], contract, preferred_element_type=f32)
        gate = lax.dot_general(normed_a, glu_gate_w[...], contract, preferred_element_type=f32)
        gated[...] = (value * jax.nn.sigmoid(gate)).astype(bf16)
        copy = tail_copy()
        copy.start()
        conv_copies.append(copy)

    def convolve():
        tail_copy().wait_recv()
        before = tail[...].astype(f32)
        padded[pl.ds(0, keep), :] = jnp.where(e > 0, before, jnp.zeros_like(before))
        padded[pl.ds(keep, taken), :] = gated[...].astype(f32)
        total = jnp.zeros((taken, chans), f32)
        for offset in range(reach + 1):
            shift = keep - reach + offset
            total = total + padded[pl.ds(shift, taken), :] * taps_ref[offset : offset + 1, :]
        done = (total + bias_ref[...]).astype(bf16)
        conv_own[...] = done
        channels[t] = done
        for o in range(1, n_tp):
            copy = pltpu.make_async_remote_copy(
                src_ref=conv_own, dst_ref=channels.at[t],
                send_sem=c_send.at[o - 1], recv_sem=c_recv.at[o - 1],
                device_id=(e, (t + o) % n_tp), device_id_type=MESH,
            )
            copy.start()
            conv_copies.append(copy)

    def mixer_end():
        for o in range(1, n_tp):
            pltpu.make_async_remote_copy(
                src_ref=conv_own, dst_ref=channels.at[(t + n_tp - o) % n_tp],
                send_sem=c_send.at[o - 1], recv_sem=c_recv.at[o - 1],
                device_id=(mate, t), device_id_type=MESH,
            ).wait_recv()
        mix_copies[3].wait()
        chan_values = jnp.concatenate([channels[i].astype(f32) for i in range(n_tp)], axis=1)
        centered = chan_values - jnp.mean(chan_values, axis=1, keepdims=True)
        variance = jnp.mean(centered * centered, axis=1, keepdims=True)
        shaped = (
            centered * lax.rsqrt(variance + norm_eps) * chan_gain_ref[...] + chan_shift_ref[...]
        )
        activated = (shaped * jax.nn.sigmoid(shaped)).astype(bf16)
        mix_out_ref[...] = jnp.dot(
            activated, mix_out_w[...], preferred_element_type=f32
        ).astype(bf16)

    glu()
    if n_z > 1:
        gather(1)
    mate_block = xin.at[rows_of(mate, cap), :]
    pltpu.make_async_remote_copy(
        src_ref=mate_block, dst_ref=mate_block, send_sem=z_send.at[0], recv_sem=z_recv.at[0],
        device_id=(mate, t), device_id_type=MESH,
    ).wait_recv()
    weight_copies[0].wait()
    weight_copies[1].wait()
    for k in range(n_z):
        if k > 0:
            gathered(k)
        up_half(k)
        if k == 0:
            weight_copies[2].wait()
        if k + 2 < n_z:
            gather(k + 2)
        down_half(k)
        if k == 0:
            convolve()
        if k > 0:
            finish(k - 1)
        if k == 1 or n_z == 1:
            mixer_end()
    finish(n_z - 1)

    block = ret.at[rows_of(mate, cap), :]
    pltpu.make_async_remote_copy(
        src_ref=block, dst_ref=block, send_sem=y_send.at[0], recv_sem=y_recv.at[0],
        device_id=(mate, t), device_id_type=MESH,
    ).wait_recv()
    for k in range(1, n_z):
        for cc in range(2):
            block = ret.at[rows_of(((z + k) % n_z) * 2 + cc, cap), :]
            pltpu.make_async_remote_copy(
                src_ref=block, dst_ref=block, send_sem=y_send.at[2 * k + cc],
                recv_sem=y_recv.at[2 * k + cc], device_id=(mate, t), device_id_type=MESH,
            ).wait_recv()
    at = lax.broadcasted_iota(jnp.int32, (rows, slots), 1)
    l0 = logits_ref[:, 0:1]
    l1 = logits_ref[:, 1:2]
    first = jnp.dot(
        (at == place0).astype(f32).astype(bf16), ret[...], preferred_element_type=f32
    )
    second = jnp.dot(
        (at == place1).astype(f32).astype(bf16), ret[...], preferred_element_type=f32
    )
    out_ref[...] = (
        first * jax.nn.sigmoid(l0 - l1) + second * jax.nn.sigmoid(l1 - l0)
    ).astype(bf16)
    for copy in [mate_copy] + z_copies + ag_copies + rs_copies + y_copies + conv_copies:
        copy.wait_send()


outer_plan = (
    "far00", "near00", "route20", "pass00", "route21", "relay20", "own00", "pass01", "relay21",
    "route30", "join20", "spread", "up20", "more20", "far20", "route10", "up10", "join21",
    "route31", "relay30", "sum01", "near20", "up21", "more21", "more10", "relay31", "far21",
    "near21", "join30", "up30", "more30", "far30", "pass20", "join31", "up31", "conv", "more31",
    "pass21", "near30", "own20", "pass30", "own21", "far31", "route11", "own30", "near31", "sum20",
    "sum21", "own31", "up11", "far10", "sum00", "more11", "sum30", "pass31", "near10", "far11",
    "own10", "pass10", "near11", "sum31", "pass11", "back2", "sum10", "back01", "own11", "sum11",
    "mix", "back3", "back00", "back1",
)
inner_plan = (
    "far00", "route20", "pass01", "near00", "relay20", "route21", "route30", "relay21", "pass00",
    "join20", "up20", "more20", "far20", "join21", "relay30", "up21", "route31", "own00", "more21",
    "far21", "near20", "join30", "pass20", "own20", "up30", "near21", "more30", "sum01", "spread",
    "sum00", "own21", "conv", "pass21", "back00", "route10", "relay31", "up10", "sum20", "more10",
    "far10", "far30", "sum21", "near30", "near10", "own30", "pass10", "join31", "up31", "own10",
    "pass30", "more31", "far31", "near31", "route11", "up11", "more11", "far11", "own31", "near11",
    "pass31", "pass11", "own11", "sum10", "sum30", "back01", "back2", "sum31", "sum11", "mix",
    "back3", "back1",
)


def paired_kernel(
    n_ep, n_tp, cap,
    x_hbm, gain_hbm, routes_hbm, logits_hbm, gate_hbm, up_hbm, down_hbm,
    mix_gain_hbm, taps_hbm, bias_hbm, chan_gain_hbm, chan_shift_hbm,
    mix_hbm, value_hbm, glu_gate_hbm, mix_out_hbm,
    out_ref, mix_out_ref,
    x_in, gain_in, routes_in, logits_in, gate_w, up_w, down_w,
    mix_gain_in, taps_in, bias_in, chan_gain_in, chan_shift_in,
    mix_in, value_w, glu_gate_w, mix_out_w,
    normed, columns, out_part, out_pair, out_near, xin, hidden_own, hidden,
    part_x, part_y, got_x, got_y, held_own, held_x, held_y, pass_x, pass_y, last_x, last_y,
    summed, ret, acc,
    load_sem, z_send, z_recv, ag_send, ag_recv, rs_send, rs_recv, y_send, y_recv,
    gated, tail, padded, conv_own, channels,
    tail_sem, c_send, c_recv,
):
    e = lax.axis_index("ep")
    t = lax.axis_index("tp")
    n_z = n_ep // 2
    z = e // 2
    c = e % 2
    mate = e + 1 - 2 * c
    rows, feat = x_in.shape
    width = ret.shape[1]
    half = width // 2
    pair = 2 * cap
    slots = n_ep * cap
    units = gate_w.shape[1]
    tile = min(units, 256)
    tiles = units // tile
    t_x = t + 1 - 2 * (t % 2)
    t_y = (t + 2) % 4
    t_d = 3 - t

    def chip_of(k):
        return [z, z + 1 - 2 * (z % 2), (z + 2) % 4, 3 - z][k]

    inner = (z + 1) // 2 % 2

    def rows_of(index, count):
        return pl.ds(pl.multiple_of(index * count, count), count)

    def cols(quarter, first, count):
        return pl.ds(pl.multiple_of(quarter * width + first, 128), count)

    def load(src, dst, at):
        return pltpu.make_async_copy(src, dst, load_sem.at[at])

    def weight_tile(j):
        here = pl.ds(pl.multiple_of(j * tile, tile), tile)
        return (
            load(gate_hbm.at[0, :, here], gate_w.at[:, here], 16 + 2 * j),
            load(up_hbm.at[0, :, here], up_w.at[:, here], 17 + 2 * j),
        )

    load_routes = load(routes_hbm, routes_in, 0)
    load_logits = load(logits_hbm, logits_in, 1)
    load_gain = load(gain_hbm, gain_in, 2)
    load_x = load(x_hbm, x_in, 3)
    load_mix = [
        load(mix_hbm, mix_in, 4), load(mix_gain_hbm, mix_gain_in, 5),
        load(value_hbm, value_w, 6), load(glu_gate_hbm, glu_gate_w, 7),
    ]
    load_conv = [load(taps_hbm, taps_in, 8), load(bias_hbm, bias_in, 9)]
    load_end = [
        load(chan_gain_hbm, chan_gain_in, 10), load(chan_shift_hbm, chan_shift_in, 11),
        load(mix_out_hbm, mix_out_w, 12),
    ]
    load_down = load(down_hbm.at[0], down_w, 13)
    for copy in [load_x, load_gain, load_routes, load_logits] + load_mix + load_conv:
        copy.start()
    for j in range(tiles):
        for copy in weight_tile(j):
            copy.start()
    for copy in [load_down] + load_end:
        copy.start()

    barrier = pltpu.get_barrier_semaphore()
    for o in range(1, n_ep):
        pl.semaphore_signal(barrier, inc=1, device_id=((e + o) % n_ep, t), device_id_type=MESH)
    for o in range(1, n_tp):
        pl.semaphore_signal(barrier, inc=1, device_id=(e, (t + o) % n_tp), device_id_type=MESH)

    load_routes.wait()
    ri = lax.broadcasted_iota(jnp.int32, (rows, rows), 0)
    ci = lax.broadcasted_iota(jnp.int32, (rows, rows), 1)
    upper = (ri < ci).astype(f32).astype(bf16)
    subs = lax.broadcasted_iota(jnp.int32, (128, rows), 0)
    t0 = (subs == routes_in[0:1, :]).astype(f32)
    t1 = (subs == routes_in[1:2, :]).astype(f32)
    count_t = jnp.dot((t0 + t1).astype(bf16), upper, preferred_element_type=f32)
    base_t = count_t + (subs * cap).astype(f32)
    place0 = jnp.sum(base_t * t0, axis=0, keepdims=True)
    place1 = jnp.sum(base_t * t1, axis=0, keepdims=True)
    row0 = place0.astype(jnp.int32)
    row1 = place1.astype(jnp.int32)

    def pick(first, size):
        at = lax.broadcasted_iota(jnp.int32, (size, rows), 0) + first
        return ((at == row0) | (at == row1)).astype(f32).astype(bf16)

    load_x.wait()
    load_gain.wait()
    values = x_in[...].astype(f32)
    scale = lax.rsqrt(jnp.mean(values * values, axis=-1, keepdims=True) + norm_eps)
    normed[...] = (values * scale * gain_in[...]).astype(bf16)
    for k in (2, 3):
        out_part[k - 2] = jnp.dot(
            pick(chip_of(k) * pair, pair), normed[:, cols(t, 0, width)],
            preferred_element_type=f32,
        ).astype(bf16)

    pl.semaphore_wait(barrier, n_ep - 1 + n_tp - 1)

    sent = []

    def send(src, dst, send_sem, recv_sem, to):
        copy = pltpu.make_async_remote_copy(
            src_ref=src, dst_ref=dst, send_sem=send_sem, recv_sem=recv_sem,
            device_id=to, device_id_type=MESH,
        )
        copy.start()
        sent.append(copy)

    def arrive(dst, send_sem, recv_sem):
        pltpu.make_async_remote_copy(
            src_ref=dst, dst_ref=dst, send_sem=send_sem, recv_sem=recv_sem,
            device_id=(mate, t), device_id_type=MESH,
        ).wait_recv()

    def core_of(h):
        return 1 - c if h else c

    def peer(k, h):
        return chip_of(k) * 2 + core_of(h)

    for k in (2, 3):
        for h in range(2):
            send(
                out_part.at[k - 2, rows_of(core_of(h), cap), :],
                xin.at[rows_of(e, cap), cols(t, 0, width)],
                z_send.at[k, h], z_recv.at[k, h], (peer(k, h), t),
            )

    out_pair[...] = jnp.dot(
        pick(mate * cap, cap), normed[...], preferred_element_type=f32
    ).astype(bf16)
    send(out_pair, xin.at[rows_of(e, cap), :], z_send.at[0, 1], z_recv.at[0, 1], (mate, t))
    for h in range(2):
        out_near[h] = jnp.dot(
            pick(peer(1, h) * cap, cap), normed[...], preferred_element_type=f32
        ).astype(bf16)
        send(
            out_near.at[h], xin.at[rows_of(e, cap), :],
            z_send.at[1, h], z_recv.at[1, h], (peer(1, h), t),
        )
    xin[rows_of(e, cap), :] = jnp.dot(
        pick(e * cap, cap), normed[...], preferred_element_type=f32
    ).astype(bf16)

    def route(k, h):
        here = rows_of(peer(k, h), cap)
        block = xin.at[here, :] if k == 1 else xin.at[here, cols(t, 0, width)]
        arrive(block, z_send.at[k, h], z_recv.at[k, h])
        if k > 1:
            send(block, block, ag_send.at[k - 2, h, 0], ag_recv.at[k - 2, h, 0], (e, t_x))
            send(block, block, ag_send.at[k - 2, h, 1], ag_recv.at[k - 2, h, 1], (e, t_y))

    def relay(k, h):
        here = rows_of(peer(k, h), cap)
        sends, recvs = ag_send.at[k - 2, h], ag_recv.at[k - 2, h]
        arrive(xin.at[here, cols(t_y, 0, width)], sends.at[1], recvs.at[1])
        block = xin.at[here, cols(t_y, 0, half)]
        send(block, block, sends.at[2], recvs.at[2], (e, t_x))
        arrive(xin.at[here, cols(t_x, 0, width)], sends.at[0], recvs.at[0])
        block = xin.at[here, cols(t_x, half, half)]
        send(block, block, sends.at[3], recvs.at[3], (e, t_y))

    def join(k, h):
        here = rows_of(peer(k, h), cap)
        sends, recvs = ag_send.at[k - 2, h], ag_recv.at[k - 2, h]
        arrive(xin.at[here, cols(t_d, 0, half)], sends.at[2], recvs.at[2])
        arrive(xin.at[here, cols(t_d, half, half)], sends.at[3], recvs.at[3])

    def gated_units(rows_in, j):
        at = pl.ds(pl.multiple_of(j * tile, tile), tile)
        g = jnp.dot(rows_in, gate_w[:, at], preferred_element_type=f32)
        u = jnp.dot(rows_in, up_w[:, at], preferred_element_type=f32)
        return at, (g * jax.nn.sigmoid(g) * u).astype(bf16)

    def up_own():
        def one(j, carry):
            for copy in weight_tile(j):
                copy.wait()
            at, block = gated_units(xin[rows_of(z, pair), :], j)
            hidden_own[:, at] = block
            return carry

        lax.fori_loop(0, tiles, one, 0)

    def up_part(k, h, first, last):
        def one(j, carry):
            at, block = gated_units(xin[rows_of(peer(k, h), cap), :], j)
            hidden[k - 1, h, :, at] = block
            return carry

        lax.fori_loop(first, last, one, 0)

    def product(k, h, quarter):
        block = hidden[k - 1, h] if k else hidden_own[rows_of(core_of(h), cap), :]
        return jnp.dot(
            block, down_w[:, cols(quarter, 0, width)], preferred_element_type=f32
        ).astype(bf16)

    def give(k, h, way, src, dst, to):
        send(src, dst, rs_send.at[k, h, way], rs_recv.at[k, h, way], (e, to))

    def down_far(k, h):
        far = product(k, h, t_d)
        part_x[k, h, 1] = far[:, :half]
        part_y[k, h, 1] = far[:, half:]
        give(k, h, 0, part_x.at[k, h, 1], got_x.at[k, h, 1], t_x)
        give(k, h, 1, part_y.at[k, h, 1], got_y.at[k, h, 1], t_y)

    def down_near(k, h):
        near = product(k, h, t_x)
        part_x[k, h, 0] = near[:, :half]
        held_x[k, h] = near[:, half:]
        give(k, h, 2, part_x.at[k, h, 0], got_x.at[k, h, 0], t_x)
        near = product(k, h, t_y)
        part_y[k, h, 0] = near[:, half:]
        held_y[k, h] = near[:, :half]
        give(k, h, 3, part_y.at[k, h, 0], got_y.at[k, h, 0], t_y)

    def down_own(k, h):
        held_own[k, h] = product(k, h, t)

    def pass_on(k, h):
        arrive(got_x.at[k, h, 1], rs_send.at[k, h, 0], rs_recv.at[k, h, 0])
        pass_y[k, h] = (held_y[k, h].astype(f32) + got_x[k, h, 1].astype(f32)).astype(bf16)
        give(k, h, 4, pass_y.at[k, h], last_y.at[k, h], t_y)
        arrive(got_y.at[k, h, 1], rs_send.at[k, h, 1], rs_recv.at[k, h, 1])
        pass_x[k, h] = (held_x[k, h].astype(f32) + got_y[k, h, 1].astype(f32)).astype(bf16)
        give(k, h, 5, pass_x.at[k, h], last_x.at[k, h], t_x)

    def finish(k, h):
        arrive(got_x.at[k, h, 0], rs_send.at[k, h, 2], rs_recv.at[k, h, 2])
        arrive(got_y.at[k, h, 0], rs_send.at[k, h, 3], rs_recv.at[k, h, 3])
        arrive(last_y.at[k, h], rs_send.at[k, h, 4], rs_recv.at[k, h, 4])
        arrive(last_x.at[k, h], rs_send.at[k, h, 5], rs_recv.at[k, h, 5])
        low = (
            held_own[k, h, :, :half].astype(f32)
            + got_x[k, h, 0].astype(f32) + last_y[k, h].astype(f32)
        ).astype(bf16)
        high = (
            held_own[k, h, :, half:].astype(f32)
            + got_y[k, h, 0].astype(f32) + last_x[k, h].astype(f32)
        ).astype(bf16)
        if k == 0 and h == 0:
            ret[rows_of(e, cap), :half] = low
            ret[rows_of(e, cap), half:] = high
            return
        summed[k, h, :, :half] = low
        summed[k, h, :, half:] = high
        send(
            summed.at[k, h], ret.at[rows_of(e, cap), :],
            y_send.at[k, h], y_recv.at[k, h], (peer(k, h), t),
        )

    def weighted(first, size):
        at = lax.broadcasted_iota(jnp.int32, (rows, size), 1) + first
        back = ret[rows_of(first // size, size), :]
        one = jnp.dot(
            (at == columns[0, :, 0:1].astype(jnp.int32)).astype(f32).astype(bf16), back,
            preferred_element_type=f32,
        )
        two = jnp.dot(
            (at == columns[1, :, 0:1].astype(jnp.int32)).astype(f32).astype(bf16), back,
            preferred_element_type=f32,
        )
        return one * columns[2, :, 0:1] + two * columns[3, :, 0:1]

    def returned(k, *part):
        for h in part or range(2):
            if k or h:
                arrive(ret.at[rows_of(peer(k, h), cap), :], y_send.at[k, h], y_recv.at[k, h])
        if part:
            return weighted(peer(k, *part) * cap, cap)
        return weighted(chip_of(k) * pair, pair)

    taken, chans = gated.shape
    keep = tail.shape[0]
    reach = taps_in.shape[0] - 1

    def tail_refs():
        return gated.at[pl.ds(taken - keep, keep), :], tail, tail_sem.at[0], tail_sem.at[1]

    def glu():
        for copy in load_mix:
            copy.wait()
        mixed = mix_in[...].astype(f32)
        inv = lax.rsqrt(jnp.mean(mixed * mixed, axis=-1, keepdims=True) + norm_eps)
        normed_a = (mixed * inv * mix_gain_in[...]).astype(bf16)
        contract = (((1,), (1,)), ((), ()))
        value = lax.dot_general(normed_a, value_w[...], contract, preferred_element_type=f32)
        gate = lax.dot_general(normed_a, glu_gate_w[...], contract, preferred_element_type=f32)
        gated[...] = (value * jax.nn.sigmoid(gate)).astype(bf16)
        send(*tail_refs(), ((e + 1) % n_ep, t))

    def convolve():
        for copy in load_conv:
            copy.wait()
        arrive(tail, tail_sem.at[0], tail_sem.at[1])
        before = tail[...].astype(f32)
        padded[pl.ds(0, keep), :] = jnp.where(e > 0, before, jnp.zeros_like(before))
        padded[pl.ds(keep, taken), :] = gated[...].astype(f32)
        total = jnp.zeros((taken, chans), f32)
        for offset in range(reach + 1):
            shift = keep - reach + offset
            total = total + padded[pl.ds(shift, taken), :] * taps_in[offset : offset + 1, :]
        done = (total + bias_in[...]).astype(bf16)
        conv_own[...] = done
        channels[t] = done
        for o in range(1, n_tp):
            send(
                conv_own, channels.at[t], c_send.at[o - 1], c_recv.at[o - 1],
                (e, (t + o) % n_tp),
            )

    def mixer_end():
        for o in range(1, n_tp):
            arrive(channels.at[(t + n_tp - o) % n_tp], c_send.at[o - 1], c_recv.at[o - 1])
        for copy in load_end:
            copy.wait()
        chan_values = jnp.concatenate([channels[i].astype(f32) for i in range(n_tp)], axis=1)
        centered = chan_values - jnp.mean(chan_values, axis=1, keepdims=True)
        variance = jnp.mean(centered * centered, axis=1, keepdims=True)
        shaped = (
            centered * lax.rsqrt(variance + norm_eps) * chan_gain_in[...] + chan_shift_in[...]
        )
        activated = (shaped * jax.nn.sigmoid(shaped)).astype(bf16)
        mix_out_ref[...] = jnp.dot(
            activated, mix_out_w[...], preferred_element_type=f32
        ).astype(bf16)

    def spread():
        load_logits.wait()
        columns[0] = jnp.broadcast_to(place0, (128, rows)).T
        columns[1] = jnp.broadcast_to(place1, (128, rows)).T
        lead = logits_in[0:1, :] - logits_in[1:2, :]
        columns[2] = jnp.broadcast_to(jax.nn.sigmoid(lead), (128, rows)).T
        columns[3] = jnp.broadcast_to(jax.nn.sigmoid(-lead), (128, rows)).T

    steps = {
        "route": route, "relay": relay, "join": join,
        "up": lambda k, h: up_part(k, h, 0, tiles // 2),
        "more": lambda k, h: up_part(k, h, tiles // 2, tiles),
        "far": down_far, "near": down_near, "own": down_own,
        "pass": pass_on, "sum": finish, "spread": spread, "conv": convolve, "mix": mixer_end,
    }

    def run(plan):
        left = sum(step.startswith("back") for step in plan)
        first = True
        for step in plan:
            name = step.rstrip("0123")
            at = [int(digit) for digit in step[len(name):]]
            with jax.named_scope(step):
                if name != "back":
                    steps[name](*at)
                    continue
                part, left = returned(*at), left - 1
                total = part if first else acc[...] + part
                first = False
                if left:
                    acc[...] = total
                else:
                    out_ref[...] = total.astype(bf16)

    with jax.named_scope("glu"):
        glu()
    with jax.named_scope("mate"):
        arrive(xin.at[rows_of(mate, cap), :], z_send.at[0, 1], z_recv.at[0, 1])
    with jax.named_scope("up_own"):
        up_own()
    load_down.wait()
    with jax.named_scope("down_own"):
        down_far(0, 1)
        down_near(0, 1)
        down_own(0, 1)
    early = len(sent)
    for side, plan in ((0, outer_plan), (1, inner_plan)):

        @pl.when(inner == side)
        def one_side(plan=plan):
            run(plan)
            for copy in sent[early:]:
                copy.wait_send()
            del sent[early:]

    for copy in sent:
        copy.wait_send()


def on_device(*args):
    n_ep, n_tp = lax.axis_size("ep"), lax.axis_size("tp")
    if n_tp == 4 and n_ep == 8:
        return paired_step(*args)
    return ring_step(*args)


def paired_step(
    mixer_input, mixer_gain, glu_value_weight, glu_gate_weight, conv_taps, conv_bias,
    channel_gain, channel_shift, mixer_out_weight, expert_input, expert_gain, routes,
    route_logits, gate_weight, up_weight, down_weight,
):
    n_ep, n_tp = lax.axis_size("ep"), lax.axis_size("tp")
    rows, feat = expert_input.shape
    cap = 3 * rows // n_ep
    cap = -(-cap // 16) * 16
    units = gate_weight.shape[2]
    width = feat // n_tp
    half = width // 2
    n_z, pair, slots = n_ep // 2, 2 * cap, n_ep * cap
    taken, chans, taps = mixer_input.shape[0], conv_taps.shape[0], conv_taps.shape[1]
    keep = -(-(taps - 1) // 16) * 16
    dma = pltpu.SemaphoreType.DMA
    operands = (
        expert_input, expert_gain[None, :], routes.T, route_logits.T,
        gate_weight, up_weight, down_weight,
        mixer_gain[None, :], conv_taps.T, conv_bias[None, :], channel_gain[None, :],
        channel_shift[None, :], mixer_input, glu_value_weight, glu_gate_weight, mixer_out_weight,
    )

    def held(array):
        shape = array.shape[1:] if array.ndim == 3 else array.shape
        return pltpu.VMEM(shape, array.dtype)

    block = pltpu.VMEM((n_z, 2, cap, half), bf16)
    blocks = pltpu.VMEM((n_z, 2, 2, cap, half), bf16)
    wide = pltpu.VMEM((n_z, 2, cap, width), bf16)
    vmem = pl.BlockSpec(memory_space=pltpu.VMEM)
    expert_output, mixer_output = pl.pallas_call(
        functools.partial(paired_kernel, n_ep, n_tp, cap),
        out_shape=(
            jax.ShapeDtypeStruct((rows, width), bf16),
            jax.ShapeDtypeStruct((taken, mixer_out_weight.shape[1]), bf16),
        ),
        in_specs=[pl.BlockSpec(memory_space=pltpu.HBM)] * len(operands),
        out_specs=(vmem, vmem),
        scratch_shapes=[held(array) for array in operands] + [
            pltpu.VMEM((rows, feat), bf16),
            pltpu.VMEM((4, rows, 128), f32),
            pltpu.VMEM((2, pair, width), bf16),
            pltpu.VMEM((cap, feat), bf16),
            pltpu.VMEM((2, cap, feat), bf16),
            pltpu.VMEM((slots, feat), bf16),
            pltpu.VMEM((pair, units), bf16),
            pltpu.VMEM((n_z - 1, 2, cap, units), bf16),
            blocks, blocks, blocks, blocks, wide, block, block, block, block, block, block,
            wide,
            pltpu.VMEM((slots, width), bf16),
            pltpu.VMEM((rows, width), f32),
            dma((16 + 2 * (units // min(units, 256)),)),
            dma((n_z, 2)),
            dma((n_z, 2)),
            dma((n_z - 2, 2, 4)),
            dma((n_z - 2, 2, 4)),
            dma((n_z, 2, 6)),
            dma((n_z, 2, 6)),
            dma((n_z, 2)),
            dma((n_z, 2)),
            pltpu.VMEM((taken, chans), bf16),
            pltpu.VMEM((keep, chans), bf16),
            pltpu.VMEM((keep + taken, chans), f32),
            pltpu.VMEM((taken, chans), bf16),
            pltpu.VMEM((n_tp, taken, chans), bf16),
            dma((2,)),
            dma((n_tp - 1,)),
            dma((n_tp - 1,)),
        ],
        compiler_params=pltpu.CompilerParams(
            collective_id=0, has_side_effects=True, vmem_limit_bytes=56 * 1024 * 1024
        ),
        cost_estimate=pl.CostEstimate(
            flops=6 * slots * feat * units, bytes_accessed=6 * feat * units, transcendentals=0
        ),
    )(*operands)
    return (mixer_output, expert_output)


def ring_step(
    mixer_input, mixer_gain, glu_value_weight, glu_gate_weight, conv_taps, conv_bias,
    channel_gain, channel_shift, mixer_out_weight, expert_input, expert_gain, routes,
    route_logits, gate_weight, up_weight, down_weight,
):
    n_ep, n_tp = lax.axis_size("ep"), lax.axis_size("tp")
    rows, feat = expert_input.shape
    cap = 3 * rows // n_ep
    cap = -(-cap // 16) * 16
    units = gate_weight.shape[2]
    width = feat // n_tp
    n_z, peers, pair, slots = n_ep // 2, n_tp - 1, 2 * cap, n_ep * cap
    taken, chans, taps = mixer_input.shape[0], conv_taps.shape[0], conv_taps.shape[1]
    keep = -(-(taps - 1) // 16) * 16
    vmem = pl.BlockSpec(memory_space=pltpu.VMEM)
    hbm = pl.BlockSpec(memory_space=pl.ANY)
    dma = pltpu.SemaphoreType.DMA
    expert_output, mixer_output = pl.pallas_call(
        functools.partial(step_kernel, n_ep, n_tp, cap),
        out_shape=(
            jax.ShapeDtypeStruct((rows, width), bf16),
            jax.ShapeDtypeStruct((taken, mixer_out_weight.shape[1]), bf16),
        ),
        in_specs=[vmem] * 5 + [hbm] * 3 + [vmem] * 5 + [hbm] * 4,
        out_specs=(vmem, vmem),
        scratch_shapes=[
            pltpu.VMEM((feat, units), bf16),
            pltpu.VMEM((feat, units), bf16),
            pltpu.VMEM((units, feat), bf16),
            pltpu.VMEM((rows, feat), bf16),
            pltpu.VMEM((slots, width), bf16),
            pltpu.VMEM((cap, feat), bf16),
            pltpu.VMEM((slots, feat), bf16),
            pltpu.VMEM((pair, units), bf16),
            pltpu.VMEM((n_z * peers, pair, width), bf16),
            pltpu.VMEM((n_z, pair, width), bf16),
            pltpu.VMEM((n_z * peers, pair, width), bf16),
            pltpu.VMEM((n_z, pair, width), bf16),
            pltpu.VMEM((slots, width), bf16),
            dma((7,)),
            dma((n_ep,)),
            dma((n_ep,)),
            dma((n_z * peers,)),
            dma((n_z * peers,)),
            dma((n_z * peers,)),
            dma((n_z * peers,)),
            dma((n_ep,)),
            dma((n_ep,)),
            pltpu.VMEM(mixer_input.shape, bf16),
            pltpu.VMEM(glu_value_weight.shape, bf16),
            pltpu.VMEM(glu_gate_weight.shape, bf16),
            pltpu.VMEM(mixer_out_weight.shape, bf16),
            pltpu.VMEM((taken, chans), bf16),
            pltpu.VMEM((keep, chans), bf16),
            pltpu.VMEM((keep + taken, chans), f32),
            pltpu.VMEM((taken, chans), bf16),
            pltpu.VMEM((n_tp, taken, chans), bf16),
            dma((2,)),
            dma((peers,)),
            dma((peers,)),
        ],
        compiler_params=pltpu.CompilerParams(
            collective_id=0, has_side_effects=True, vmem_limit_bytes=48 * 1024 * 1024
        ),
        cost_estimate=pl.CostEstimate(
            flops=6 * slots * feat * units, bytes_accessed=6 * feat * units, transcendentals=0
        ),
    )(
        expert_input, expert_gain[None, :], routes, routes.T, route_logits,
        gate_weight, up_weight, down_weight,
        mixer_gain[None, :], conv_taps.T, conv_bias[None, :], channel_gain[None, :],
        channel_shift[None, :], mixer_input, glu_value_weight, glu_gate_weight, mixer_out_weight,
    )
    return (mixer_output, expert_output)


def solution(mesh):
    in_specs = (
        P("ep", None),
        P(),
        P("tp", None),
        P("tp", None),
        P("tp", None),
        P("tp"),
        P(),
        P(),
        P(None, "tp"),
        P("ep", None),
        P(),
        P("ep", None),
        P("ep", None),
        P("ep", None, "tp"),
        P("ep", None, "tp"),
        P("ep", "tp", None),
    )
    out_specs = (P("ep", "tp"), P("ep", "tp"))
    return jax.shard_map(
        on_device, mesh=mesh, in_specs=in_specs, out_specs=out_specs, check_vma=False
    )
```

```python
import functools

import jax
import jax.numpy as jnp
from jax import lax
from jax.experimental import pallas as pl
from jax.experimental.pallas import tpu as pltpu
from jax.sharding import PartitionSpec as P

norm_eps = 1e-06
MESH = pl.DeviceIdType.MESH
f32 = jnp.float32
bf16 = jnp.bfloat16


def step_kernel(
    n_ep, n_tp, cap,
    x_ref, gain_ref, routes_ref, routes_t_ref, logits_ref, gate_hbm, up_hbm, down_hbm,
    mix_gain_ref, taps_ref, bias_ref, chan_gain_ref, chan_shift_ref,
    mix_hbm, value_hbm, glu_gate_hbm, mix_out_hbm,
    out_ref, mix_out_ref,
    gate_w, up_w, down_w, normed, out_part, out_pair, xin, hidden, part, own_part, got, summed, ret,
    w_sem, z_send, z_recv, ag_send, ag_recv, rs_send, rs_recv, y_send, y_recv,
    mix_in, value_w, glu_gate_w, mix_out_w, gated, tail, padded, conv_own, channels,
    tail_sem, c_send, c_recv,
):
    e = lax.axis_index("ep")
    t = lax.axis_index("tp")
    n_z = n_ep // 2
    z = e // 2
    c = e % 2
    mate = e + 1 - 2 * c
    width = out_part.shape[1]
    rows, feat = x_ref.shape
    pair = 2 * cap
    slots = n_ep * cap
    peers = n_tp - 1

    weight_copies = [
        pltpu.make_async_copy(gate_hbm.at[0], gate_w, w_sem.at[0]),
        pltpu.make_async_copy(up_hbm.at[0], up_w, w_sem.at[1]),
        pltpu.make_async_copy(down_hbm.at[0], down_w, w_sem.at[2]),
    ]
    mix_copies = [
        pltpu.make_async_copy(mix_hbm, mix_in, w_sem.at[3]),
        pltpu.make_async_copy(value_hbm, value_w, w_sem.at[4]),
        pltpu.make_async_copy(glu_gate_hbm, glu_gate_w, w_sem.at[5]),
        pltpu.make_async_copy(mix_out_hbm, mix_out_w, w_sem.at[6]),
    ]
    for copy in mix_copies[:3] + weight_copies + mix_copies[3:]:
        copy.start()

    barrier = pltpu.get_barrier_semaphore()
    for o in range(1, n_ep):
        pl.semaphore_signal(barrier, inc=1, device_id=((e + o) % n_ep, t), device_id_type=MESH)
    for o in range(1, n_tp):
        pl.semaphore_signal(barrier, inc=1, device_id=(e, (t + o) % n_tp), device_id_type=MESH)

    def rows_of(index, count):
        return pl.ds(pl.multiple_of(index * count, count), count)

    def cols_of(index, count):
        return pl.ds(pl.multiple_of(index * count, count), count)

    values = x_ref[...].astype(f32)
    scale = lax.rsqrt(jnp.mean(values * values, axis=-1, keepdims=True) + norm_eps)
    normed[...] = (values * scale * gain_ref[...]).astype(bf16)

    lanes = lax.broadcasted_iota(jnp.int32, (rows, 128), 1)
    m0 = (lanes == routes_ref[:, 0:1]).astype(f32)
    m1 = (lanes == routes_ref[:, 1:2]).astype(f32)
    ri = lax.broadcasted_iota(jnp.int32, (rows, rows), 0)
    ci = lax.broadcasted_iota(jnp.int32, (rows, rows), 1)
    lower = (ci < ri).astype(f32).astype(bf16)
    upper = (ri < ci).astype(f32).astype(bf16)
    count = jnp.dot(lower, (m0 + m1).astype(bf16), preferred_element_type=f32)
    base = count + (lanes * cap).astype(f32)
    place0 = jnp.sum(base * m0, axis=1, keepdims=True).astype(jnp.int32)
    place1 = jnp.sum(base * m1, axis=1, keepdims=True).astype(jnp.int32)
    subs = lax.broadcasted_iota(jnp.int32, (128, rows), 0)
    t0 = (subs == routes_t_ref[0:1, :]).astype(f32)
    t1 = (subs == routes_t_ref[1:2, :]).astype(f32)
    count_t = jnp.dot((t0 + t1).astype(bf16), upper, preferred_element_type=f32)
    base_t = count_t + (subs * cap).astype(f32)
    row0 = jnp.sum(base_t * t0, axis=0, keepdims=True).astype(jnp.int32)
    row1 = jnp.sum(base_t * t1, axis=0, keepdims=True).astype(jnp.int32)

    def pick(first, size):
        at = lax.broadcasted_iota(jnp.int32, (size, rows), 0) + first
        return ((at == row0) | (at == row1)).astype(f32).astype(bf16)

    out_part[...] = jnp.dot(
        pick(0, slots), normed[:, cols_of(t, width)], preferred_element_type=f32
    ).astype(bf16)

    pl.semaphore_wait(barrier, n_ep - 1 + peers)

    z_copies = []
    for k in range(1, n_z):
        for cc in range(2):
            dest = ((z + k) % n_z) * 2 + cc
            copy = pltpu.make_async_remote_copy(
                src_ref=out_part.at[rows_of(dest, cap), :],
                dst_ref=xin.at[rows_of(e, cap), cols_of(t, width)],
                send_sem=z_send.at[2 * k + cc],
                recv_sem=z_recv.at[2 * k + c],
                device_id=(dest, t),
                device_id_type=MESH,
            )
            copy.start()
            z_copies.append(copy)

    out_pair[...] = jnp.dot(
        pick(mate * cap, cap), normed[...], preferred_element_type=f32
    ).astype(bf16)
    mate_copy = pltpu.make_async_remote_copy(
        src_ref=out_pair,
        dst_ref=xin.at[rows_of(e, cap), :],
        send_sem=z_send.at[0],
        recv_sem=z_recv.at[0],
        device_id=(mate, t),
        device_id_type=MESH,
    )
    mate_copy.start()
    xin[rows_of(e, cap), :] = jnp.dot(
        pick(e * cap, cap), normed[...], preferred_element_type=f32
    ).astype(bf16)

    def source_chip(k):
        return (z + n_z - k) % n_z

    ag_copies = []

    def gather(k):
        chip = source_chip(k)
        for cc in range(2):
            block = xin.at[rows_of(chip * 2 + cc, cap), cols_of(t, width)]
            pltpu.make_async_remote_copy(
                src_ref=block, dst_ref=block, send_sem=z_send.at[2 * k + cc],
                recv_sem=z_recv.at[2 * k + cc], device_id=(mate, t), device_id_type=MESH,
            ).wait_recv()
        block = xin.at[rows_of(chip, pair), cols_of(t, width)]
        for o in range(1, n_tp):
            copy = pltpu.make_async_remote_copy(
                src_ref=block, dst_ref=block, send_sem=ag_send.at[k * peers + o - 1],
                recv_sem=ag_recv.at[k * peers + o - 1],
                device_id=(e, (t + o) % n_tp), device_id_type=MESH,
            )
            copy.start()
            ag_copies.append(copy)

    def gathered(k):
        chip = source_chip(k)
        for o in range(1, n_tp):
            block = xin.at[rows_of(chip, pair), cols_of((t + n_tp - o) % n_tp, width)]
            pltpu.make_async_remote_copy(
                src_ref=block, dst_ref=block, send_sem=ag_send.at[k * peers + o - 1],
                recv_sem=ag_recv.at[k * peers + o - 1],
                device_id=(mate, t), device_id_type=MESH,
            ).wait_recv()

    units = gate_w.shape[1]
    tile = min(units, 256)
    rs_copies = []
    y_copies = []

    def up_half(k):
        here = rows_of(source_chip(k), pair)

        def one(j, carry):
            cols = cols_of(j, tile)
            rows_in = xin[here, :]
            g = jnp.dot(rows_in, gate_w[:, cols], preferred_element_type=f32)
            u = jnp.dot(rows_in, up_w[:, cols], preferred_element_type=f32)
            hidden[:, cols] = (g * jax.nn.sigmoid(g) * u).astype(bf16)
            return carry

        lax.fori_loop(0, units // tile, one, 0)

    def down_half(k):
        for o in range(1, n_tp):
            peer = (t + o) % n_tp
            at = k * peers + o - 1
            part[at] = jnp.dot(
                hidden[...], down_w[:, cols_of(peer, width)], preferred_element_type=f32
            ).astype(bf16)
            copy = pltpu.make_async_remote_copy(
                src_ref=part.at[at], dst_ref=got.at[at], send_sem=rs_send.at[at],
                recv_sem=rs_recv.at[at], device_id=(e, peer), device_id_type=MESH,
            )
            copy.start()
            rs_copies.append(copy)
        own_part[k] = jnp.dot(
            hidden[...], down_w[:, cols_of(t, width)], preferred_element_type=f32
        ).astype(bf16)

    def finish(k):
        chip = source_chip(k)
        total = own_part[k].astype(f32)
        for o in range(1, n_tp):
            at = k * peers + o - 1
            pltpu.make_async_remote_copy(
                src_ref=part.at[at], dst_ref=got.at[at], send_sem=rs_send.at[at],
                recv_sem=rs_recv.at[at], device_id=(mate, t), device_id_type=MESH,
            ).wait_recv()
            total = total + got[at].astype(f32)
        summed[k] = total.astype(bf16)
        if k == 0:
            copy = pltpu.make_async_remote_copy(
                src_ref=summed.at[0, rows_of(1 - c, cap), :], dst_ref=ret.at[rows_of(e, cap), :],
                send_sem=y_send.at[0], recv_sem=y_recv.at[0],
                device_id=(mate, t), device_id_type=MESH,
            )
            copy.start()
            y_copies.append(copy)
            ret[rows_of(e, cap), :] = summed[0, rows_of(c, cap), :]
            return
        for cc in range(2):
            copy = pltpu.make_async_remote_copy(
                src_ref=summed.at[k, pl.ds(cc * cap, cap), :], dst_ref=ret.at[rows_of(e, cap), :],
                send_sem=y_send.at[2 * k + cc], recv_sem=y_recv.at[2 * k + c],
                device_id=(chip * 2 + cc, t), device_id_type=MESH,
            )
            copy.start()
            y_copies.append(copy)

    taken, chans = gated.shape
    keep = tail.shape[0]
    reach = taps_ref.shape[0] - 1
    conv_copies = []

    def tail_copy():
        return pltpu.make_async_remote_copy(
            src_ref=gated.at[pl.ds(taken - keep, keep), :], dst_ref=tail,
            send_sem=tail_sem.at[0], recv_sem=tail_sem.at[1],
            device_id=((e + 1) % n_ep, t), device_id_type=MESH,
        )

    def glu():
        for copy in mix_copies[:3]:
            copy.wait()
        mixed = mix_in[...].astype(f32)
        inv = lax.rsqrt(jnp.mean(mixed * mixed, axis=-1, keepdims=True) + norm_eps)
        normed_a = (mixed * inv * mix_gain_ref[...]).astype(bf16)
        contract = (((1,), (1,)), ((), ()))
        value = lax.dot_general(normed_a, value_w[...], contract, preferred_element_type=f32)
        gate = lax.dot_general(normed_a, glu_gate_w[...], contract, preferred_element_type=f32)
        gated[...] = (value * jax.nn.sigmoid(gate)).astype(bf16)
        copy = tail_copy()
        copy.start()
        conv_copies.append(copy)

    def convolve():
        tail_copy().wait_recv()
        before = tail[...].astype(f32)
        padded[pl.ds(0, keep), :] = jnp.where(e > 0, before, jnp.zeros_like(before))
        padded[pl.ds(keep, taken), :] = gated[...].astype(f32)
        total = jnp.zeros((taken, chans), f32)
        for offset in range(reach + 1):
            shift = keep - reach + offset
            total = total + padded[pl.ds(shift, taken), :] * taps_ref[offset : offset + 1, :]
        done = (total + bias_ref[...]).astype(bf16)
        conv_own[...] = done
        channels[t] = done
        for o in range(1, n_tp):
            copy = pltpu.make_async_remote_copy(
                src_ref=conv_own, dst_ref=channels.at[t],
                send_sem=c_send.at[o - 1], recv_sem=c_recv.at[o - 1],
                device_id=(e, (t + o) % n_tp), device_id_type=MESH,
            )
            copy.start()
            conv_copies.append(copy)

    def mixer_end():
        for o in range(1, n_tp):
            pltpu.make_async_remote_copy(
                src_ref=conv_own, dst_ref=channels.at[(t + n_tp - o) % n_tp],
                send_sem=c_send.at[o - 1], recv_sem=c_recv.at[o - 1],
                device_id=(mate, t), device_id_type=MESH,
            ).wait_recv()
        mix_copies[3].wait()
        chan_values = jnp.concatenate([channels[i].astype(f32) for i in range(n_tp)], axis=1)
        centered = chan_values - jnp.mean(chan_values, axis=1, keepdims=True)
        variance = jnp.mean(centered * centered, axis=1, keepdims=True)
        shaped = (
            centered * lax.rsqrt(variance + norm_eps) * chan_gain_ref[...] + chan_shift_ref[...]
        )
        activated = (shaped * jax.nn.sigmoid(shaped)).astype(bf16)
        mix_out_ref[...] = jnp.dot(
            activated, mix_out_w[...], preferred_element_type=f32
        ).astype(bf16)

    glu()
    if n_z > 1:
        gather(1)
    mate_block = xin.at[rows_of(mate, cap), :]
    pltpu.make_async_remote_copy(
        src_ref=mate_block, dst_ref=mate_block, send_sem=z_send.at[0], recv_sem=z_recv.at[0],
        device_id=(mate, t), device_id_type=MESH,
    ).wait_recv()
    weight_copies[0].wait()
    weight_copies[1].wait()
    for k in range(n_z):
        if k > 0:
            gathered(k)
        up_half(k)
        if k == 0:
            weight_copies[2].wait()
        if k + 2 < n_z:
            gather(k + 2)
        down_half(k)
        if k == 0:
            convolve()
        if k > 0:
            finish(k - 1)
        if k == 1 or n_z == 1:
            mixer_end()
    finish(n_z - 1)

    block = ret.at[rows_of(mate, cap), :]
    pltpu.make_async_remote_copy(
        src_ref=block, dst_ref=block, send_sem=y_send.at[0], recv_sem=y_recv.at[0],
        device_id=(mate, t), device_id_type=MESH,
    ).wait_recv()
    for k in range(1, n_z):
        for cc in range(2):
            block = ret.at[rows_of(((z + k) % n_z) * 2 + cc, cap), :]
            pltpu.make_async_remote_copy(
                src_ref=block, dst_ref=block, send_sem=y_send.at[2 * k + cc],
                recv_sem=y_recv.at[2 * k + cc], device_id=(mate, t), device_id_type=MESH,
            ).wait_recv()
    at = lax.broadcasted_iota(jnp.int32, (rows, slots), 1)
    l0 = logits_ref[:, 0:1]
    l1 = logits_ref[:, 1:2]
    first = jnp.dot(
        (at == place0).astype(f32).astype(bf16), ret[...], preferred_element_type=f32
    )
    second = jnp.dot(
        (at == place1).astype(f32).astype(bf16), ret[...], preferred_element_type=f32
    )
    out_ref[...] = (
        first * jax.nn.sigmoid(l0 - l1) + second * jax.nn.sigmoid(l1 - l0)
    ).astype(bf16)
    for copy in [mate_copy] + z_copies + ag_copies + rs_copies + y_copies + conv_copies:
        copy.wait_send()


outer_plan = (
    "far00", "near00", "route20", "pass00", "route21", "relay20", "own00", "pass01", "relay21",
    "route30", "join20", "spread", "up20", "more20", "far20", "route10", "up10", "join21",
    "route31", "relay30", "sum01", "near20", "up21", "more21", "more10", "relay31", "far21",
    "near21", "join30", "up30", "more30", "far30", "pass20", "join31", "up31", "conv", "more31",
    "pass21", "near30", "own20", "pass30", "own21", "far31", "route11", "own30", "near31", "sum20",
    "sum21", "own31", "up11", "far10", "sum00", "more11", "sum30", "pass31", "near10", "far11",
    "own10", "pass10", "near11", "sum31", "pass11", "back2", "sum10", "back01", "own11", "sum11",
    "mix", "back3", "back00", "back1",
)
inner_plan = (
    "far00", "route20", "pass01", "near00", "relay20", "route21", "route30", "relay21", "pass00",
    "join20", "up20", "more20", "far20", "join21", "relay30", "up21", "route31", "own00", "more21",
    "far21", "near20", "join30", "pass20", "own20", "up30", "near21", "more30", "sum01", "spread",
    "sum00", "own21", "conv", "pass21", "back00", "route10", "relay31", "up10", "sum20", "more10",
    "far10", "far30", "sum21", "near30", "near10", "own30", "pass10", "join31", "up31", "own10",
    "pass30", "more31", "far31", "near31", "route11", "up11", "more11", "far11", "own31", "near11",
    "pass31", "pass11", "own11", "sum10", "sum30", "back01", "back2", "sum31", "sum11", "mix",
    "back3", "back1",
)


def paired_kernel(
    n_ep, n_tp, cap,
    x_hbm, gain_hbm, routes_hbm, logits_hbm, gate_hbm, up_hbm, down_hbm,
    mix_gain_hbm, taps_hbm, bias_hbm, chan_gain_hbm, chan_shift_hbm,
    mix_hbm, value_hbm, glu_gate_hbm, mix_out_hbm,
    out_ref, mix_out_ref,
    x_in, gain_in, routes_in, logits_in, gate_w, up_w, down_w,
    mix_gain_in, taps_in, bias_in, chan_gain_in, chan_shift_in,
    mix_in, value_w, glu_gate_w, mix_out_w,
    normed, columns, out_part, out_pair, out_near, xin, hidden_own, hidden,
    part_x, part_y, got_x, got_y, held_own, held_x, held_y, pass_x, pass_y, last_x, last_y,
    summed, ret, acc,
    load_sem, z_send, z_recv, ag_send, ag_recv, rs_send, rs_recv, y_send, y_recv,
    gated, tail, padded, conv_own, channels,
    tail_sem, c_send, c_recv,
):
    e = lax.axis_index("ep")
    t = lax.axis_index("tp")
    n_z = n_ep // 2
    z = e // 2
    c = e % 2
    mate = e + 1 - 2 * c
    rows, feat = x_in.shape
    width = ret.shape[1]
    half = width // 2
    pair = 2 * cap
    slots = n_ep * cap
    units = gate_w.shape[1]
    tile = min(units, 256)
    tiles = units // tile
    t_x = t + 1 - 2 * (t % 2)
    t_y = (t + 2) % 4
    t_d = 3 - t

    def chip_of(k):
        return [z, z + 1 - 2 * (z % 2), (z + 2) % 4, 3 - z][k]

    inner = (z + 1) // 2 % 2

    def rows_of(index, count):
        return pl.ds(pl.multiple_of(index * count, count), count)

    def cols(quarter, first, count):
        return pl.ds(pl.multiple_of(quarter * width + first, 128), count)

    def load(src, dst, at):
        return pltpu.make_async_copy(src, dst, load_sem.at[at])

    def weight_tile(j):
        here = pl.ds(pl.multiple_of(j * tile, tile), tile)
        return (
            load(gate_hbm.at[0, :, here], gate_w.at[:, here], 16 + 2 * j),
            load(up_hbm.at[0, :, here], up_w.at[:, here], 17 + 2 * j),
        )

    load_routes = load(routes_hbm, routes_in, 0)
    load_logits = load(logits_hbm, logits_in, 1)
    load_gain = load(gain_hbm, gain_in, 2)
    load_x = load(x_hbm, x_in, 3)
    load_mix = [
        load(mix_hbm, mix_in, 4), load(mix_gain_hbm, mix_gain_in, 5),
        load(value_hbm, value_w, 6), load(glu_gate_hbm, glu_gate_w, 7),
    ]
    load_conv = [load(taps_hbm, taps_in, 8), load(bias_hbm, bias_in, 9)]
    load_end = [
        load(chan_gain_hbm, chan_gain_in, 10), load(chan_shift_hbm, chan_shift_in, 11),
        load(mix_out_hbm, mix_out_w, 12),
    ]
    load_down = load(down_hbm.at[0], down_w, 13)
    for copy in [load_x, load_gain, load_routes, load_logits] + load_mix + load_conv:
        copy.start()
    for j in range(tiles):
        for copy in weight_tile(j):
            copy.start()
    for copy in [load_down] + load_end:
        copy.start()

    barrier = pltpu.get_barrier_semaphore()
    for o in range(1, n_ep):
        pl.semaphore_signal(barrier, inc=1, device_id=((e + o) % n_ep, t), device_id_type=MESH)
    for o in range(1, n_tp):
        pl.semaphore_signal(barrier, inc=1, device_id=(e, (t + o) % n_tp), device_id_type=MESH)

    load_routes.wait()
    ri = lax.broadcasted_iota(jnp.int32, (rows, rows), 0)
    ci = lax.broadcasted_iota(jnp.int32, (rows, rows), 1)
    upper = (ri < ci).astype(f32).astype(bf16)
    subs = lax.broadcasted_iota(jnp.int32, (128, rows), 0)
    t0 = (subs == routes_in[0:1, :]).astype(f32)
    t1 = (subs == routes_in[1:2, :]).astype(f32)
    count_t = jnp.dot((t0 + t1).astype(bf16), upper, preferred_element_type=f32)
    base_t = count_t + (subs * cap).astype(f32)
    place0 = jnp.sum(base_t * t0, axis=0, keepdims=True)
    place1 = jnp.sum(base_t * t1, axis=0, keepdims=True)
    row0 = place0.astype(jnp.int32)
    row1 = place1.astype(jnp.int32)

    def pick(first, size):
        at = lax.broadcasted_iota(jnp.int32, (size, rows), 0) + first
        return ((at == row0) | (at == row1)).astype(f32).astype(bf16)

    load_x.wait()
    load_gain.wait()
    values = x_in[...].astype(f32)
    scale = lax.rsqrt(jnp.mean(values * values, axis=-1, keepdims=True) + norm_eps)
    normed[...] = (values * scale * gain_in[...]).astype(bf16)
    for k in (2, 3):
        out_part[k - 2] = jnp.dot(
            pick(chip_of(k) * pair, pair), normed[:, cols(t, 0, width)],
            preferred_element_type=f32,
        ).astype(bf16)

    pl.semaphore_wait(barrier, n_ep - 1 + n_tp - 1)

    sent = []

    def send(src, dst, send_sem, recv_sem, to):
        copy = pltpu.make_async_remote_copy(
            src_ref=src, dst_ref=dst, send_sem=send_sem, recv_sem=recv_sem,
            device_id=to, device_id_type=MESH,
        )
        copy.start()
        sent.append(copy)

    def arrive(dst, send_sem, recv_sem):
        pltpu.make_async_remote_copy(
            src_ref=dst, dst_ref=dst, send_sem=send_sem, recv_sem=recv_sem,
            device_id=(mate, t), device_id_type=MESH,
        ).wait_recv()

    def core_of(h):
        return 1 - c if h else c

    def peer(k, h):
        return chip_of(k) * 2 + core_of(h)

    for k in (2, 3):
        for h in range(2):
            send(
                out_part.at[k - 2, rows_of(core_of(h), cap), :],
                xin.at[rows_of(e, cap), cols(t, 0, width)],
                z_send.at[k, h], z_recv.at[k, h], (peer(k, h), t),
            )

    out_pair[...] = jnp.dot(
        pick(mate * cap, cap), normed[...], preferred_element_type=f32
    ).astype(bf16)
    send(out_pair, xin.at[rows_of(e, cap), :], z_send.at[0, 1], z_recv.at[0, 1], (mate, t))
    for h in range(2):
        out_near[h] = jnp.dot(
            pick(peer(1, h) * cap, cap), normed[...], preferred_element_type=f32
        ).astype(bf16)
        send(
            out_near.at[h], xin.at[rows_of(e, cap), :],
            z_send.at[1, h], z_recv.at[1, h], (peer(1, h), t),
        )
    xin[rows_of(e, cap), :] = jnp.dot(
        pick(e * cap, cap), normed[...], preferred_element_type=f32
    ).astype(bf16)

    def route(k, h):
        here = rows_of(peer(k, h), cap)
        block = xin.at[here, :] if k == 1 else xin.at[here, cols(t, 0, width)]
        arrive(block, z_send.at[k, h], z_recv.at[k, h])
        if k > 1:
            send(block, block, ag_send.at[k - 2, h, 0], ag_recv.at[k - 2, h, 0], (e, t_x))
            send(block, block, ag_send.at[k - 2, h, 1], ag_recv.at[k - 2, h, 1], (e, t_y))

    def relay(k, h):
        here = rows_of(peer(k, h), cap)
        sends, recvs = ag_send.at[k - 2, h], ag_recv.at[k - 2, h]
        arrive(xin.at[here, cols(t_y, 0, width)], sends.at[1], recvs.at[1])
        block = xin.at[here, cols(t_y, 0, half)]
        send(block, block, sends.at[2], recvs.at[2], (e, t_x))
        arrive(xin.at[here, cols(t_x, 0, width)], sends.at[0], recvs.at[0])
        block = xin.at[here, cols(t_x, half, half)]
        send(block, block, sends.at[3], recvs.at[3], (e, t_y))

    def join(k, h):
        here = rows_of(peer(k, h), cap)
        sends, recvs = ag_send.at[k - 2, h], ag_recv.at[k - 2, h]
        arrive(xin.at[here, cols(t_d, 0, half)], sends.at[2], recvs.at[2])
        arrive(xin.at[here, cols(t_d, half, half)], sends.at[3], recvs.at[3])

    def gated_units(rows_in, j):
        at = pl.ds(pl.multiple_of(j * tile, tile), tile)
        g = jnp.dot(rows_in, gate_w[:, at], preferred_element_type=f32)
        u = jnp.dot(rows_in, up_w[:, at], preferred_element_type=f32)
        return at, (g * jax.nn.sigmoid(g) * u).astype(bf16)

    def up_own():
        def one(j, carry):
            for copy in weight_tile(j):
                copy.wait()
            at, block = gated_units(xin[rows_of(z, pair), :], j)
            hidden_own[:, at] = block
            return carry

        lax.fori_loop(0, tiles, one, 0)

    def up_part(k, h, first, last):
        def one(j, carry):
            at, block = gated_units(xin[rows_of(peer(k, h), cap), :], j)
            hidden[k - 1, h, :, at] = block
            return carry

        lax.fori_loop(first, last, one, 0)

    def product(k, h, quarter):
        block = hidden[k - 1, h] if k else hidden_own[rows_of(core_of(h), cap), :]
        return jnp.dot(
            block, down_w[:, cols(quarter, 0, width)], preferred_element_type=f32
        ).astype(bf16)

    def give(k, h, way, src, dst, to):
        send(src, dst, rs_send.at[k, h, way], rs_recv.at[k, h, way], (e, to))

    def down_far(k, h):
        far = product(k, h, t_d)
        part_x[k, h, 1] = far[:, :half]
        part_y[k, h, 1] = far[:, half:]
        give(k, h, 0, part_x.at[k, h, 1], got_x.at[k, h, 1], t_x)
        give(k, h, 1, part_y.at[k, h, 1], got_y.at[k, h, 1], t_y)

    def down_near(k, h):
        near = product(k, h, t_x)
        part_x[k, h, 0] = near[:, :half]
        held_x[k, h] = near[:, half:]
        give(k, h, 2, part_x.at[k, h, 0], got_x.at[k, h, 0], t_x)
        near = product(k, h, t_y)
        part_y[k, h, 0] = near[:, half:]
        held_y[k, h] = near[:, :half]
        give(k, h, 3, part_y.at[k, h, 0], got_y.at[k, h, 0], t_y)

    def down_own(k, h):
        held_own[k, h] = product(k, h, t)

    def pass_on(k, h):
        arrive(got_x.at[k, h, 1], rs_send.at[k, h, 0], rs_recv.at[k, h, 0])
        pass_y[k, h] = (held_y[k, h].astype(f32) + got_x[k, h, 1].astype(f32)).astype(bf16)
        give(k, h, 4, pass_y.at[k, h], last_y.at[k, h], t_y)
        arrive(got_y.at[k, h, 1], rs_send.at[k, h, 1], rs_recv.at[k, h, 1])
        pass_x[k, h] = (held_x[k, h].astype(f32) + got_y[k, h, 1].astype(f32)).astype(bf16)
        give(k, h, 5, pass_x.at[k, h], last_x.at[k, h], t_x)

    def finish(k, h):
        arrive(got_x.at[k, h, 0], rs_send.at[k, h, 2], rs_recv.at[k, h, 2])
        arrive(got_y.at[k, h, 0], rs_send.at[k, h, 3], rs_recv.at[k, h, 3])
        arrive(last_y.at[k, h], rs_send.at[k, h, 4], rs_recv.at[k, h, 4])
        arrive(last_x.at[k, h], rs_send.at[k, h, 5], rs_recv.at[k, h, 5])
        low = (
            held_own[k, h, :, :half].astype(f32)
            + got_x[k, h, 0].astype(f32) + last_y[k, h].astype(f32)
        ).astype(bf16)
        high = (
            held_own[k, h, :, half:].astype(f32)
            + got_y[k, h, 0].astype(f32) + last_x[k, h].astype(f32)
        ).astype(bf16)
        if k == 0 and h == 0:
            ret[rows_of(e, cap), :half] = low
            ret[rows_of(e, cap), half:] = high
            return
        summed[k, h, :, :half] = low
        summed[k, h, :, half:] = high
        send(
            summed.at[k, h], ret.at[rows_of(e, cap), :],
            y_send.at[k, h], y_recv.at[k, h], (peer(k, h), t),
        )

    def weighted(first, size):
        at = lax.broadcasted_iota(jnp.int32, (rows, size), 1) + first
        back = ret[rows_of(first // size, size), :]
        one = jnp.dot(
            (at == columns[0, :, 0:1].astype(jnp.int32)).astype(f32).astype(bf16), back,
            preferred_element_type=f32,
        )
        two = jnp.dot(
            (at == columns[1, :, 0:1].astype(jnp.int32)).astype(f32).astype(bf16), back,
            preferred_element_type=f32,
        )
        return one * columns[2, :, 0:1] + two * columns[3, :, 0:1]

    def returned(k, *part):
        for h in part or range(2):
            if k or h:
                arrive(ret.at[rows_of(peer(k, h), cap), :], y_send.at[k, h], y_recv.at[k, h])
        if part:
            return weighted(peer(k, *part) * cap, cap)
        return weighted(chip_of(k) * pair, pair)

    taken, chans = gated.shape
    keep = tail.shape[0]
    reach = taps_in.shape[0] - 1

    def tail_refs():
        return gated.at[pl.ds(taken - keep, keep), :], tail, tail_sem.at[0], tail_sem.at[1]

    def glu():
        for copy in load_mix:
            copy.wait()
        mixed = mix_in[...].astype(f32)
        inv = lax.rsqrt(jnp.mean(mixed * mixed, axis=-1, keepdims=True) + norm_eps)
        normed_a = (mixed * inv * mix_gain_in[...]).astype(bf16)
        contract = (((1,), (1,)), ((), ()))
        value = lax.dot_general(normed_a, value_w[...], contract, preferred_element_type=f32)
        gate = lax.dot_general(normed_a, glu_gate_w[...], contract, preferred_element_type=f32)
        gated[...] = (value * jax.nn.sigmoid(gate)).astype(bf16)
        send(*tail_refs(), ((e + 1) % n_ep, t))

    def convolve():
        for copy in load_conv:
            copy.wait()
        arrive(tail, tail_sem.at[0], tail_sem.at[1])
        before = tail[...].astype(f32)
        padded[pl.ds(0, keep), :] = jnp.where(e > 0, before, jnp.zeros_like(before))
        padded[pl.ds(keep, taken), :] = gated[...].astype(f32)
        total = jnp.zeros((taken, chans), f32)
        for offset in range(reach + 1):
            shift = keep - reach + offset
            total = total + padded[pl.ds(shift, taken), :] * taps_in[offset : offset + 1, :]
        done = (total + bias_in[...]).astype(bf16)
        conv_own[...] = done
        channels[t] = done
        for o in range(1, n_tp):
            send(
                conv_own, channels.at[t], c_send.at[o - 1], c_recv.at[o - 1],
                (e, (t + o) % n_tp),
            )

    def mixer_end():
        for o in range(1, n_tp):
            arrive(channels.at[(t + n_tp - o) % n_tp], c_send.at[o - 1], c_recv.at[o - 1])
        for copy in load_end:
            copy.wait()
        chan_values = jnp.concatenate([channels[i].astype(f32) for i in range(n_tp)], axis=1)
        centered = chan_values - jnp.mean(chan_values, axis=1, keepdims=True)
        variance = jnp.mean(centered * centered, axis=1, keepdims=True)
        shaped = (
            centered * lax.rsqrt(variance + norm_eps) * chan_gain_in[...] + chan_shift_in[...]
        )
        activated = (shaped * jax.nn.sigmoid(shaped)).astype(bf16)
        mix_out_ref[...] = jnp.dot(
            activated, mix_out_w[...], preferred_element_type=f32
        ).astype(bf16)

    def spread():
        load_logits.wait()
        columns[0] = jnp.broadcast_to(place0, (128, rows)).T
        columns[1] = jnp.broadcast_to(place1, (128, rows)).T
        lead = logits_in[0:1, :] - logits_in[1:2, :]
        columns[2] = jnp.broadcast_to(jax.nn.sigmoid(lead), (128, rows)).T
        columns[3] = jnp.broadcast_to(jax.nn.sigmoid(-lead), (128, rows)).T

    steps = {
        "route": route, "relay": relay, "join": join,
        "up": lambda k, h: up_part(k, h, 0, tiles // 2),
        "more": lambda k, h: up_part(k, h, tiles // 2, tiles),
        "far": down_far, "near": down_near, "own": down_own,
        "pass": pass_on, "sum": finish, "spread": spread, "conv": convolve, "mix": mixer_end,
    }

    def run(plan):
        left = sum(step.startswith("back") for step in plan)
        first = True
        for step in plan:
            name = step.rstrip("0123")
            at = [int(digit) for digit in step[len(name):]]
            with jax.named_scope(step):
                if name != "back":
                    steps[name](*at)
                    continue
                part, left = returned(*at), left - 1
                total = part if first else acc[...] + part
                first = False
                if left:
                    acc[...] = total
                else:
                    out_ref[...] = total.astype(bf16)

    with jax.named_scope("glu"):
        glu()
    with jax.named_scope("mate"):
        arrive(xin.at[rows_of(mate, cap), :], z_send.at[0, 1], z_recv.at[0, 1])
    with jax.named_scope("up_own"):
        up_own()
    load_down.wait()
    with jax.named_scope("down_own"):
        down_far(0, 1)
        down_near(0, 1)
        down_own(0, 1)
    early = len(sent)
    for side, plan in ((0, outer_plan), (1, inner_plan)):

        @pl.when(inner == side)
        def one_side(plan=plan):
            run(plan)
            for copy in sent[early:]:
                copy.wait_send()
            del sent[early:]

    for copy in sent:
        copy.wait_send()


def on_device(*args):
    n_ep, n_tp = lax.axis_size("ep"), lax.axis_size("tp")
    if n_tp == 4 and n_ep == 8:
        return paired_step(*args)
    return ring_step(*args)


def paired_step(
    mixer_input, mixer_gain, glu_value_weight, glu_gate_weight, conv_taps, conv_bias,
    channel_gain, channel_shift, mixer_out_weight, expert_input, expert_gain, routes,
    route_logits, gate_weight, up_weight, down_weight,
):
    n_ep, n_tp = lax.axis_size("ep"), lax.axis_size("tp")
    rows, feat = expert_input.shape
    cap = 3 * rows // n_ep
    cap = -(-cap // 16) * 16
    units = gate_weight.shape[2]
    width = feat // n_tp
    half = width // 2
    n_z, pair, slots = n_ep // 2, 2 * cap, n_ep * cap
    taken, chans, taps = mixer_input.shape[0], conv_taps.shape[0], conv_taps.shape[1]
    keep = -(-(taps - 1) // 16) * 16
    dma = pltpu.SemaphoreType.DMA
    operands = (
        expert_input, expert_gain[None, :], routes.T, route_logits.T,
        gate_weight, up_weight, down_weight,
        mixer_gain[None, :], conv_taps.T, conv_bias[None, :], channel_gain[None, :],
        channel_shift[None, :], mixer_input, glu_value_weight, glu_gate_weight, mixer_out_weight,
    )

    def held(array):
        shape = array.shape[1:] if array.ndim == 3 else array.shape
        return pltpu.VMEM(shape, array.dtype)

    block = pltpu.VMEM((n_z, 2, cap, half), bf16)
    blocks = pltpu.VMEM((n_z, 2, 2, cap, half), bf16)
    wide = pltpu.VMEM((n_z, 2, cap, width), bf16)
    vmem = pl.BlockSpec(memory_space=pltpu.VMEM)
    expert_output, mixer_output = pl.pallas_call(
        functools.partial(paired_kernel, n_ep, n_tp, cap),
        out_shape=(
            pltpu.VMEM((rows, width), bf16),
            pltpu.VMEM((taken, mixer_out_weight.shape[1]), bf16),
        ),
        in_specs=[pl.BlockSpec(memory_space=pltpu.HBM)] * len(operands),
        out_specs=(vmem, vmem),
        scratch_shapes=[held(array) for array in operands] + [
            pltpu.VMEM((rows, feat), bf16),
            pltpu.VMEM((4, rows, 128), f32),
            pltpu.VMEM((2, pair, width), bf16),
            pltpu.VMEM((cap, feat), bf16),
            pltpu.VMEM((2, cap, feat), bf16),
            pltpu.VMEM((slots, feat), bf16),
            pltpu.VMEM((pair, units), bf16),
            pltpu.VMEM((n_z - 1, 2, cap, units), bf16),
            blocks, blocks, blocks, blocks, wide, block, block, block, block, block, block,
            wide,
            pltpu.VMEM((slots, width), bf16),
            pltpu.VMEM((rows, width), f32),
            dma((16 + 2 * (units // min(units, 256)),)),
            dma((n_z, 2)),
            dma((n_z, 2)),
            dma((n_z - 2, 2, 4)),
            dma((n_z - 2, 2, 4)),
            dma((n_z, 2, 6)),
            dma((n_z, 2, 6)),
            dma((n_z, 2)),
            dma((n_z, 2)),
            pltpu.VMEM((taken, chans), bf16),
            pltpu.VMEM((keep, chans), bf16),
            pltpu.VMEM((keep + taken, chans), f32),
            pltpu.VMEM((taken, chans), bf16),
            pltpu.VMEM((n_tp, taken, chans), bf16),
            dma((2,)),
            dma((n_tp - 1,)),
            dma((n_tp - 1,)),
        ],
        compiler_params=pltpu.CompilerParams(
            collective_id=0, has_side_effects=True, vmem_limit_bytes=56 * 1024 * 1024
        ),
        cost_estimate=pl.CostEstimate(
            flops=6 * slots * feat * units, bytes_accessed=6 * feat * units, transcendentals=0
        ),
    )(*operands)
    return (mixer_output, expert_output)


def ring_step(
    mixer_input, mixer_gain, glu_value_weight, glu_gate_weight, conv_taps, conv_bias,
    channel_gain, channel_shift, mixer_out_weight, expert_input, expert_gain, routes,
    route_logits, gate_weight, up_weight, down_weight,
):
    n_ep, n_tp = lax.axis_size("ep"), lax.axis_size("tp")
    rows, feat = expert_input.shape
    cap = 3 * rows // n_ep
    cap = -(-cap // 16) * 16
    units = gate_weight.shape[2]
    width = feat // n_tp
    n_z, peers, pair, slots = n_ep // 2, n_tp - 1, 2 * cap, n_ep * cap
    taken, chans, taps = mixer_input.shape[0], conv_taps.shape[0], conv_taps.shape[1]
    keep = -(-(taps - 1) // 16) * 16
    vmem = pl.BlockSpec(memory_space=pltpu.VMEM)
    hbm = pl.BlockSpec(memory_space=pl.ANY)
    dma = pltpu.SemaphoreType.DMA
    expert_output, mixer_output = pl.pallas_call(
        functools.partial(step_kernel, n_ep, n_tp, cap),
        out_shape=(
            jax.ShapeDtypeStruct((rows, width), bf16),
            jax.ShapeDtypeStruct((taken, mixer_out_weight.shape[1]), bf16),
        ),
        in_specs=[vmem] * 5 + [hbm] * 3 + [vmem] * 5 + [hbm] * 4,
        out_specs=(vmem, vmem),
        scratch_shapes=[
            pltpu.VMEM((feat, units), bf16),
            pltpu.VMEM((feat, units), bf16),
            pltpu.VMEM((units, feat), bf16),
            pltpu.VMEM((rows, feat), bf16),
            pltpu.VMEM((slots, width), bf16),
            pltpu.VMEM((cap, feat), bf16),
            pltpu.VMEM((slots, feat), bf16),
            pltpu.VMEM((pair, units), bf16),
            pltpu.VMEM((n_z * peers, pair, width), bf16),
            pltpu.VMEM((n_z, pair, width), bf16),
            pltpu.VMEM((n_z * peers, pair, width), bf16),
            pltpu.VMEM((n_z, pair, width), bf16),
            pltpu.VMEM((slots, width), bf16),
            dma((7,)),
            dma((n_ep,)),
            dma((n_ep,)),
            dma((n_z * peers,)),
            dma((n_z * peers,)),
            dma((n_z * peers,)),
            dma((n_z * peers,)),
            dma((n_ep,)),
            dma((n_ep,)),
            pltpu.VMEM(mixer_input.shape, bf16),
            pltpu.VMEM(glu_value_weight.shape, bf16),
            pltpu.VMEM(glu_gate_weight.shape, bf16),
            pltpu.VMEM(mixer_out_weight.shape, bf16),
            pltpu.VMEM((taken, chans), bf16),
            pltpu.VMEM((keep, chans), bf16),
            pltpu.VMEM((keep + taken, chans), f32),
            pltpu.VMEM((taken, chans), bf16),
            pltpu.VMEM((n_tp, taken, chans), bf16),
            dma((2,)),
            dma((peers,)),
            dma((peers,)),
        ],
        compiler_params=pltpu.CompilerParams(
            collective_id=0, has_side_effects=True, vmem_limit_bytes=48 * 1024 * 1024
        ),
        cost_estimate=pl.CostEstimate(
            flops=6 * slots * feat * units, bytes_accessed=6 * feat * units, transcendentals=0
        ),
    )(
        expert_input, expert_gain[None, :], routes, routes.T, route_logits,
        gate_weight, up_weight, down_weight,
        mixer_gain[None, :], conv_taps.T, conv_bias[None, :], channel_gain[None, :],
        channel_shift[None, :], mixer_input, glu_value_weight, glu_gate_weight, mixer_out_weight,
    )
    return (mixer_output, expert_output)


def solution(mesh):
    in_specs = (
        P("ep", None),
        P(),
        P("tp", None),
        P("tp", None),
        P("tp", None),
        P("tp"),
        P(),
        P(),
        P(None, "tp"),
        P("ep", None),
        P(),
        P("ep", None),
        P("ep", None),
        P("ep", None, "tp"),
        P("ep", None, "tp"),
        P("ep", "tp", None),
    )
    out_specs = (P("ep", "tp"), P("ep", "tp"))
    return jax.shard_map(
        on_device, mesh=mesh, in_specs=in_specs, out_specs=out_specs, check_vma=False
    )
```
